256 devices in a mesh: sp: 64 (over z, y, core), tp: 4 (over x).
Axes of the slice: x: 4, y: 4, z: 8, core: 2. Of those that a mesh axis runs over, the one named last changes fastest.
Arguments:
- resid: bfloat16 [16384, 2048], P(('sp', 'tp')), may hold values from -6 to 6
- queries: bfloat16 [16384, 1024], P('sp', 'tp'), may hold values from -6 to 6
- keys: bfloat16 [16384, 256], P('sp', 'tp'), may hold values from -6 to 6
- values: bfloat16 [16384, 256], P('sp', 'tp'), may hold values from -6 to 6
- docs: int32 [16384], P('sp'), may hold values from 0 to 31, never falling along the last dimension, each value on 1 to 1024 neighbouring positions
- q_gain: float32 [64], replicated, may hold values from 0.1 to 1.9
- key_norm_gain: float32 [64], replicated, may hold values from 0.1 to 1.9
- sink: float32 [16], P('tp'), may hold values from 4 to 8
- out_gain: float32 [1024], replicated, may hold values from 0.1 to 1.9
- w_out: bfloat16 [1024, 2048], replicated, may hold values from -0.1875 to 0.1875
- norm_gain: float32 [2048], replicated, may hold values from 0.1 to 1.9
- routes: int32 [16384, 4], P('sp'), may hold values from 0 to 63, all different within a row; in each aligned block of 64 rows (0 to 63, 64 to 127, ...) at most 8 rows name the same one
- route_weights: float32 [16384, 4], P(('sp', 'tp')), may hold values from 0.1 to 1
- w_gate: bfloat16 [64, 2048, 2048], P('sp', None, 'tp'), may hold values from -0.375 to 0.375
- w_up: bfloat16 [64, 2048, 2048], P('sp', None, 'tp'), may hold values from -0.375 to 0.375
- w_down: bfloat16 [64, 2048, 2048], P('sp', 'tp'), may hold values from -0.015625 to 0.015625
Outputs:
- layer_out: bfloat16 [16384, 2048], P(('sp', 'tp'))
The draws below stay inside these ranges and needn't reach their ends.
Inputs may be any that keep to these rules, and one draw needn't show every extreme that they name: `routes`: in each aligned block of 64 tokens no expert is named more than 8 times, and some expert is named exactly that often; the 4 experts of a token differ. `docs`: document numbers never fall along the sequence, and each document has 1 to 1024 positions.
All inputs are finite; a program needn't handle non-finite values.
Results may differ from the reference program's by a relative error of at most 0.015.
Values may be sent and summed in bfloat16 or wider, within the bound.
A program may use at most 128 MiB of HBM per device.

```python
import math
import jax
import jax.numpy as jnp
import numpy as np
from jax import lax

D = 2048
QUERY_HEAD_COUNT = 16
KEY_VALUE_HEADS = 4
HEAD_DIMENSION = 64
ATT = 1024
FF = 2048
EXPERTS = 64
TOP = 4
WINDOW = 128
TOK_DEV = 256
PACKED_TOKENS = 16384
TQ = 64
CAP_SLOT = 8
DOCS = 32
DOC_SPAN = 1024
N_SP = 64
N_TP = 4


def block_levels(own_key, shape, shards, least, largest):
    def one(dim, blocks):
        steps = jax.random.uniform(jax.random.fold_in(jax.random.fold_in(own_key, 6), dim), (blocks,), jnp.float32, least / len(shards), largest / len(shards))
        return jnp.repeat(jnp.exp(steps), shape[dim] // blocks).reshape((-1,) + (1,) * (len(shape) - dim - 1))

    gain = one(*shards[0])
    for cut in shards[1:]:
        gain = gain * one(*cut)
    return gain


def split_up(count, total, reach, skew):
    weights = [(1 << 20) // math.isqrt(rank ** skew) + 1 for rank in range(2, count + 1)]
    spare, counts = total - reach - (count - 1), [1] * (count - 1)
    while spare > 0:
        candidates = [i for i in range(count - 1) if counts[i] < reach]
        pool, left = sum([weights[i] for i in candidates]), spare
        for i in candidates:
            addition = min(reach - counts[i], max(1, left * weights[i] // pool), spare)
            counts[i] = counts[i] + addition
            spare = spare - addition
    return np.array([reach] + counts)


def uneven_parts(key, number_of, total, reach, skew):
    if number_of == 2:
        one = jax.random.randint(key, (), max(1, total - reach), min(reach, total - 1) + 1)
        return jnp.stack([one, total - one])
    lengths = jnp.asarray(split_up(number_of, total, reach, skew), jnp.int32)
    twos = (number_of - 1) // 2
    giver, taker = lengths[1:1 + 2 * twos:2], lengths[2:2 + 2 * twos:2]
    margin = jnp.minimum(giver - 1, reach - taker)
    shifted = jax.random.randint(jax.random.fold_in(key, 1), (twos,), 0, 1 << 20) % (margin + 1)
    lengths = lengths.at[1:1 + 2 * twos:2].set(giver - shifted).at[2:2 + 2 * twos:2].set(taker + shifted)
    return lengths[jax.random.permutation(jax.random.fold_in(key, 2), number_of)]


def routed_block(own_key, own, number, rows, number_of, top, most, slope):
    ranking = jax.random.permutation(own_key, number_of)
    crowded, common = load_shares(number_of, rows * top, most, slope, True), load_shares(number_of, rows * top, most, slope, False)
    places = jnp.arange(number_of)

    def named(lengths, offset_by):
        used = int((lengths > 0).sum())
        fixed = max(1, used // 4)
        passed = fixed + (places - fixed + offset_by * (used - fixed)) % max(1, number_of - fixed)
        return jnp.zeros((number_of,), jnp.int32).at[ranking[jnp.where(places < fixed, places, passed)]].set(jnp.asarray(lengths, jnp.int32))

    lengths = jnp.where(number % 4 == 0, named(crowded, number // 4), named(common, number - number // 4 - 1))
    mixed = jax.random.permutation(jax.random.fold_in(own, 3), number_of)
    donor, taker = mixed[0:number_of // 2 * 2:2], mixed[1:number_of // 2 * 2:2]
    room = jnp.minimum(lengths[donor] - 1, most - lengths[taker]) // 2
    room = jnp.where((donor == ranking[0]) | (taker == ranking[0]) | (lengths[taker] == 0), 0, jnp.maximum(room, 0))
    passed = jax.random.randint(jax.random.fold_in(own, 4), (number_of // 2,), 0, 1 << 20) % (room + 1)
    lengths = lengths.at[donor].add(-passed).at[taker].add(passed)
    items = jnp.searchsorted(jnp.cumsum(lengths), jnp.arange(rows * top), side="right").astype(jnp.int32)
    grid = items.reshape(top, rows).T
    grid = grid[jax.random.permutation(jax.random.fold_in(own, 1), rows)]
    offset_by = jax.random.randint(jax.random.fold_in(own, 2), (rows, 1), 0, top)
    return jnp.take_along_axis(grid, (jnp.arange(top)[None, :] + offset_by) % top, axis=1)


def load_shares(count, total, limit, lean, full):
    loads = [(1 << 20) // math.isqrt(rank ** lean) + 1 for rank in range(1, count + 1)]
    largest = limit if full else min(limit, max(-(-total // count), total * loads[0] // sum(loads)))
    least = 1 if total - largest >= count - 1 else 0
    counts, rest = [largest] + [least] * (count - 1), total - largest - least * (count - 1)
    while rest > 0:
        candidates = [i for i in range(1, count) if counts[i] < largest] or [i for i in range(1, count) if counts[i] < limit]
        mass, remaining = sum([loads[i] for i in candidates]), rest
        for i in candidates:
            addition = min(limit - counts[i], max(1, remaining * loads[i] // mass), rest)
            counts[i] = counts[i] + addition
            rest = rest - addition
    return np.array(counts)


def gaussian(rng, shape, spread, bound, shards=(), kind=jnp.bfloat16):
    level = block_levels(rng, shape, shards, -0.22, 0.18) if shards else 1.0
    array = jax.random.normal(rng, shape, jnp.float32) * spread * level
    return jnp.minimum(jnp.maximum(array, -bound), bound).astype(kind)


def setup_inputs(seed: int = 0) -> dict:
    arg_keys = jax.random.split(jax.random.key(seed), 17)
    resid = gaussian(arg_keys[0], (PACKED_TOKENS, D), 1.0, 6.0, ((0, 256),))
    queries = gaussian(arg_keys[1], (PACKED_TOKENS, ATT), 1.0, 6.0, ((0, 64), (1, 4)))
    keys = gaussian(arg_keys[2], (PACKED_TOKENS, KEY_VALUE_HEADS * HEAD_DIMENSION), 1.0, 6.0, ((0, 64), (1, 4)))
    values = gaussian(arg_keys[3], (PACKED_TOKENS, KEY_VALUE_HEADS * HEAD_DIMENSION), 1.0, 6.0, ((0, 64), (1, 4)))
    docs = jnp.searchsorted(jnp.cumsum(uneven_parts(arg_keys[4], DOCS, PACKED_TOKENS, DOC_SPAN, 2)), jnp.arange(PACKED_TOKENS), side="right").astype(jnp.int32)
    q_gain = jnp.clip(1.0 + 0.18 * jax.random.normal(arg_keys[5], (HEAD_DIMENSION,), jnp.float32), 0.1, 1.9)
    key_norm_gain = jnp.clip(1.0 + 0.18 * jax.random.normal(arg_keys[6], (HEAD_DIMENSION,), jnp.float32), 0.1, 1.9)
    sink = jnp.clip(4.0 + 4.0 * jax.random.uniform(arg_keys[7], (QUERY_HEAD_COUNT,), jnp.float32) ** block_levels(arg_keys[7], (QUERY_HEAD_COUNT,), ((0, 4),), -0.2, 0.2), 4.0, 8.0)
    out_gain = jnp.clip(1.0 + 0.18 * jax.random.normal(arg_keys[8], (ATT,), jnp.float32), 0.1, 1.9)
    w_out = gaussian(arg_keys[9], (ATT, D), ATT ** -0.5, 0.1875)
    norm_gain = jnp.clip(1.0 + 0.18 * jax.random.normal(arg_keys[10], (D,), jnp.float32), 0.1, 1.9)
    routes_keys = jax.random.split(jax.random.fold_in(arg_keys[11], 1), PACKED_TOKENS // TQ)
    routes_turns = jax.random.permutation(jax.random.fold_in(arg_keys[11], 3), PACKED_TOKENS // TQ)
    routes = jax.vmap(lambda own, number: routed_block(jax.random.fold_in(arg_keys[11], 2), own, number, TQ, EXPERTS, TOP, CAP_SLOT, 2))(routes_keys, routes_turns).reshape((PACKED_TOKENS, TOP))
    route_weights = jnp.clip(0.1 + 0.9 * jax.random.uniform(arg_keys[12], (PACKED_TOKENS, TOP), jnp.float32) ** block_levels(arg_keys[12], (PACKED_TOKENS, TOP), ((0, 256),), -0.2, 0.2), 0.1, 1.0)
    w_gate = gaussian(arg_keys[13], (EXPERTS, D, FF), (D // 9) ** -0.5, 0.375, ((0, 64), (2, 4)))
    w_up = gaussian(arg_keys[14], (EXPERTS, D, FF), (D // 9) ** -0.5, 0.375, ((0, 64), (2, 4)))
    w_down = gaussian(arg_keys[15], (EXPERTS, FF, D), (64 * FF) ** -0.5, 0.015625, ((0, 64), (1, 4)))
    return dict(resid=resid, queries=queries, keys=keys, values=values, docs=docs, q_gain=q_gain, key_norm_gain=key_norm_gain, sink=sink, out_gain=out_gain, w_out=w_out, norm_gain=norm_gain, routes=routes, route_weights=route_weights, w_gate=w_gate, w_up=w_up, w_down=w_down)


rope_base = 10000.0
norm_eps = 1e-06
swiglu_limit = 7.0
swiglu_alpha = 1.702

def row_normalize(values, gain_vec):
    floats = values.astype(jnp.float32)
    scale_inv = lax.rsqrt(lax.optimization_barrier(jnp.mean(floats * floats, axis=-1, keepdims=True)) + norm_eps)
    return floats * scale_inv * gain_vec.astype(jnp.float32)

def apply_rotary_heads(heads, token_positions):
    half_size = heads.shape[-1] // 2
    freqs = rope_base ** (-jnp.arange(half_size, dtype=jnp.float32) / half_size)
    angles = token_positions[:, None] * freqs[None, :]
    cosine = jnp.cos(angles)[:, None, :]
    sine = jnp.sin(angles)[:, None, :]
    first_half = heads[..., :half_size]
    second_half = heads[..., half_size:]
    return jnp.concatenate([first_half * cosine - second_half * sine, first_half * sine + second_half * cosine], axis=-1)

def expert_act(gate_pre, up_pre):
    gate_cut = jnp.minimum(gate_pre, swiglu_limit)
    up_cut = jnp.clip(up_pre, -swiglu_limit, swiglu_limit)
    return (up_cut + 1.0) * gate_cut * jax.nn.sigmoid(swiglu_alpha * gate_cut)

def slot_tables(route_block, expert_count, capacity):
    pair_total = route_block.shape[1]
    expert_ids = jnp.arange(expert_count, dtype=jnp.int32)
    onehot = (route_block[:, :, None] == expert_ids[None, None, :]).astype(jnp.int32)
    before = jnp.cumsum(onehot, axis=1).astype(jnp.int32) - onehot
    rank = lax.optimization_barrier(jnp.sum(before * onehot, axis=-1)).astype(jnp.int32)
    pair_slot = (route_block * capacity + rank).astype(jnp.int32)
    slot_ids = jnp.arange(expert_count * capacity, dtype=jnp.int32)
    match = pair_slot[:, :, None] == slot_ids[None, None, :]
    pair_ids = jnp.arange(pair_total, dtype=jnp.int32)
    slot_pair = lax.optimization_barrier(jnp.sum(jnp.where(match, pair_ids[None, :, None], 0), axis=1)).astype(jnp.int32)
    filled = jnp.any(match, axis=1)
    return (pair_slot, slot_pair, filled)

def reference(resid, queries, keys, values, docs, q_gain, key_norm_gain, sink, out_gain, w_out, norm_gain, routes, route_weights, w_gate, w_up, w_down):
    query_group_width = QUERY_HEAD_COUNT // KEY_VALUE_HEADS
    token_positions = jnp.arange(PACKED_TOKENS, dtype=jnp.float32)
    q_rot = apply_rotary_heads(row_normalize(queries.reshape(PACKED_TOKENS, QUERY_HEAD_COUNT, HEAD_DIMENSION), q_gain), token_positions).astype(jnp.bfloat16)
    key_rotated = apply_rotary_heads(row_normalize(keys.reshape(PACKED_TOKENS, KEY_VALUE_HEADS, HEAD_DIMENSION), key_norm_gain), token_positions).astype(jnp.bfloat16)
    value_head_rows = values.reshape(PACKED_TOKENS, KEY_VALUE_HEADS, HEAD_DIMENSION)
    k_pad = jnp.pad(key_rotated, ((WINDOW, WINDOW), (0, 0), (0, 0)))
    v_pad = jnp.pad(value_head_rows, ((WINDOW, WINDOW), (0, 0), (0, 0)))
    doc_pad = jnp.pad(docs, (WINDOW, WINDOW), constant_values=-1)
    block_row_list = math.gcd(512, PACKED_TOKENS)
    span_rows = block_row_list + 2 * WINDOW
    scale = HEAD_DIMENSION ** (-0.5)
    sink_exponent = jnp.exp(sink.astype(jnp.float32)).reshape(KEY_VALUE_HEADS, query_group_width)

    def attend(block_id):
        first_row = (block_id * block_row_list).astype(jnp.int32)
        query_block_tile = lax.dynamic_slice_in_dim(q_rot, first_row, block_row_list, 0)
        query_block_tile = query_block_tile.reshape(block_row_list, KEY_VALUE_HEADS, query_group_width, HEAD_DIMENSION).astype(jnp.float32)
        k_block = lax.dynamic_slice_in_dim(k_pad, first_row, span_rows, 0).astype(jnp.float32)
        v_block = lax.dynamic_slice_in_dim(v_pad, first_row, span_rows, 0).astype(jnp.float32)
        doc_query = lax.dynamic_slice_in_dim(docs, first_row, block_row_list, 0)
        doc_key = lax.dynamic_slice_in_dim(doc_pad, first_row, span_rows, 0)
        scores = jnp.einsum('qhgd,khd->hgqk', query_block_tile, k_block) * scale
        offsets = jnp.arange(block_row_list, dtype=jnp.int32)[:, None] - (jnp.arange(span_rows, dtype=jnp.int32)[None, :] - WINDOW)
        allowed = (jnp.abs(offsets) <= WINDOW) & (doc_query[:, None] == doc_key[None, :])
        raw_weights = jnp.where(allowed[None, None], jnp.exp(scores), jnp.zeros((), jnp.float32))
        total = lax.optimization_barrier(jnp.sum(raw_weights, axis=-1)) + sink_exponent[:, :, None]
        probs = (raw_weights / total[..., None]).astype(jnp.bfloat16)
        mixed = jnp.einsum('hgqk,khd->qhgd', probs.astype(jnp.float32), v_block)
        return mixed.reshape(block_row_list, QUERY_HEAD_COUNT * HEAD_DIMENSION).astype(jnp.bfloat16)
    att = lax.map(attend, jnp.arange(PACKED_TOKENS // block_row_list, dtype=jnp.int32)).reshape(PACKED_TOKENS, QUERY_HEAD_COUNT * HEAD_DIMENSION)
    att_normed = row_normalize(att, out_gain).astype(jnp.bfloat16)
    middle = (resid.astype(jnp.float32) + jnp.dot(att_normed, w_out, preferred_element_type=jnp.float32)).astype(jnp.bfloat16)
    moe_in = row_normalize(middle, norm_gain).astype(jnp.bfloat16)
    quarter = TOK_DEV // N_TP
    block_count = N_SP * N_TP
    pair_total = quarter * TOP
    pair_slot, slot_pair, filled = slot_tables(routes.reshape(block_count, pair_total), EXPERTS, CAP_SLOT)
    slot_pair = slot_pair.reshape(block_count, EXPERTS, CAP_SLOT).transpose(1, 0, 2)
    filled = filled.reshape(block_count, EXPERTS, CAP_SLOT).transpose(1, 0, 2)
    block_base = (jnp.arange(block_count, dtype=jnp.int32) * quarter)[:, None]
    hidden_group = FF // N_TP

    def one_expert(accum, inputs):
        pair_ids, used, gate_w, up_w, down_w = inputs
        token_ids = (block_base + pair_ids // TOP).reshape(-1).astype(jnp.int32)
        route_slot = (pair_ids % TOP).reshape(-1).astype(jnp.int32)
        rows_in = moe_in[token_ids]
        gate_pre = jnp.dot(rows_in, gate_w, preferred_element_type=jnp.float32)
        up_pre = jnp.dot(rows_in, up_w, preferred_element_type=jnp.float32)
        hidden = expert_act(gate_pre, up_pre).astype(jnp.bfloat16)
        summed = jnp.zeros((rows_in.shape[0], D), jnp.float32)
        for group_id in range(N_TP):
            part = jnp.dot(hidden[:, group_id * hidden_group:(group_id + 1) * hidden_group], down_w[group_id * hidden_group:(group_id + 1) * hidden_group], preferred_element_type=jnp.float32)
            summed = summed + lax.optimization_barrier(part.astype(jnp.bfloat16)).astype(jnp.float32)
        expert_out = lax.optimization_barrier(summed.astype(jnp.bfloat16)).astype(jnp.float32)
        weight = route_weights[token_ids, route_slot] * used.reshape(-1).astype(jnp.float32)
        accum = accum.at[token_ids].add(weight[:, None] * expert_out)
        return (accum, None)
    accum, unused = lax.scan(one_expert, jnp.zeros((PACKED_TOKENS, D), jnp.float32), (slot_pair, filled, w_gate, w_up, w_down))
    return (middle.astype(jnp.float32) + accum).astype(jnp.bfloat16)
```

```python
import jax
import jax.numpy as jnp
from jax import lax
from jax.experimental import pallas as pl
from jax.experimental.pallas import tpu as pltpu
from jax.sharding import PartitionSpec as P

WINDOW = 128
MESH = pl.DeviceIdType.MESH

NZ = 8
PLANE = 8
NX = 4
CAP = 8
CHUNKS = 8
WIDE = ()


rope_base = 10000.0
norm_eps = 1e-06
swiglu_limit = 7.0
swiglu_alpha = 1.702
VMEM_LIMIT = 63 * 1024 * 1024


def extended(x, sides, width):
    for axis, dim in sides:
        peers, length = (lax.axis_size(axis), x.shape[dim])
        up = [(i, (i + 1) % peers) for i in range(peers - 1)]
        down = [(j, i) for i, j in up]
        last = lax.slice_in_dim(x, length - width, length, axis=dim)
        leading = lax.slice_in_dim(x, 0, width, axis=dim)
        before = lax.ppermute(last, axis, up)
        after = lax.ppermute(leading, axis, down)
        x = jnp.concatenate([before, x, after], axis=dim)
    return x


def row_normalize(values, gain_vec):
    floats = values.astype(jnp.float32)
    scale_inv = lax.rsqrt(jnp.mean(floats * floats, axis=-1, keepdims=True) + norm_eps)
    return floats * scale_inv * gain_vec


def apply_rotary_heads(heads, token_positions):
    half_size = heads.shape[-1] // 2
    freqs = rope_base ** (-jnp.arange(half_size, dtype=jnp.float32) / half_size)
    angles = token_positions[:, None] * freqs[None, :]
    cosine = jnp.cos(angles)[:, None, :]
    sine = jnp.sin(angles)[:, None, :]
    first_half = heads[..., :half_size]
    second_half = heads[..., half_size:]
    return jnp.concatenate(
        [first_half * cosine - second_half * sine, first_half * sine + second_half * cosine],
        axis=-1,
    )


class Net:
    def __init__(self, sems):
        self.sems = sems
        self.used = 0
        self.copies = {}

    def send(self, name, src, dst, device):
        copy = pltpu.make_async_remote_copy(
            src_ref=src,
            dst_ref=dst,
            send_sem=self.sems.at[self.used],
            recv_sem=self.sems.at[self.used + 1],
            device_id=device,
            device_id_type=MESH,
        )
        self.used += 2
        copy.start()
        self.copies[name] = [copy, False]

    def arrived(self, name):
        self.copies[name][0].wait_recv()

    def sent(self, name):
        if not self.copies[name][1]:
            self.copies[name][0].wait_send()
            self.copies[name][1] = True


def moe_kernel(
    tok_ref, meta_ref, mid_ref, wg_hbm, wu_hbm, wd_hbm, out_ref,
    wg, wu, wd, rows, gate_acc, up_acc, hidden, meta, pick, mix_hi, mix_lo,
    scr_narrow, scr_wide, sems, wsem,
):
    bf16, f32 = jnp.bfloat16, jnp.float32
    width = tok_ref.shape[1] // CHUNKS
    toks = tok_ref.shape[0]
    block = PLANE * toks
    half = block // 2
    sp, x = lax.axis_index("sp"), lax.axis_index("tp")
    z, p = sp // PLANE, lax.rem(sp, PLANE)
    z_up = lax.rem(z + 1, NZ) * PLANE + p
    z_down = lax.rem(z + NZ - 1, NZ) * PLANE + p
    x_up, x_down, x_far = lax.rem(x + 1, NX), lax.rem(x + NX - 1, NX), lax.rem(x + 2, NX)
    up, down = (z_up, x), (z_down, x)
    right, left, far = (sp, x_up), (sp, x_down), (sp, x_far)
    ahead = [(z * PLANE + lax.rem(p + q, PLANE), x) for q in range(PLANE)]
    behind = [(z * PLANE + lax.rem(p + PLANE - q, PLANE), x) for q in range(PLANE)]
    net = Net(sems)
    narrow = [k for k in range(CHUNKS) if k not in WIDE]
    place = {k: (scr_wide, WIDE.index(k), NX) if k in WIDE else (scr_narrow, narrow.index(k), 1) for k in range(CHUNKS)}

    def buf(k, name):
        group, i, _ = place[k]
        return group[name].at[i]

    def cols(k):
        return slice(k * width, (k + 1) * width)

    weight_copies = [
        pltpu.make_async_copy(src.at[0], dst, wsem.at[i])
        for i, (src, dst) in enumerate(((wg_hbm, wg), (wu_hbm, wu), (wd_hbm, wd)))
    ]
    for copy in weight_copies:
        copy.start()

    barrier = pltpu.get_barrier_semaphore()
    peers = [up, down, right, left] + ahead[1:] + ([far] if WIDE else [])
    for peer in peers:
        pl.semaphore_signal(barrier, inc=1, device_id=peer, device_id_type=MESH)
    pl.semaphore_wait(barrier, len(peers))

    meta_width = NX if WIDE else 1

    def up_hops(k):
        return 4 if k % 2 == 0 else 3

    def up_slot(h):
        return h

    def down_slot(h):
        return 4 if h == 4 else (0 if h == 0 else 4 + h)

    def own_tokens(k):
        spread = buf(k, "spread")
        spread[0, 0] = tok_ref[:, cols(k)]

    def wide_first(k):
        spread = buf(k, "spread")
        src = tok_ref.at[:, cols(k)]
        net.send((k, "w", 1), src, spread.at[0, 1], right)
        net.send((k, "w", 2), src, spread.at[0, 2], left)
        net.send((k, "w", 3), src, spread.at[0, 3], far)

    def meta_first():
        meta[0, 0] = meta_ref[...]
        if WIDE:
            net.send(("mw", 1), meta_ref, meta.at[0, 1], right)
            net.send(("mw", 2), meta_ref, meta.at[0, 2], left)
            net.send(("mw", 3), meta_ref, meta.at[0, 3], far)

    def ring_hop(name, h, last_up, last_down, data):
        if h <= last_up:
            if h > 1:
                net.arrived((name, "u", h - 1))
            net.send((name, "u", h), data.at[up_slot(h - 1)], data.at[up_slot(h)], up)
        if h <= last_down:
            if h > 1:
                net.arrived((name, "d", h - 1))
            net.send((name, "d", h), data.at[down_slot(h - 1)], data.at[down_slot(h)], down)

    def meta_hop(h):
        if h == 1 and WIDE:
            for i in (1, 2, 3):
                net.arrived(("mw", i))
        ring_hop("m", h, 4, 3, meta)

    def token_hop(k, h):
        if h == 1 and k in WIDE:
            for i in (1, 2, 3):
                net.arrived((k, "w", i))
        ring_hop(k, h, up_hops(k), 7 - up_hops(k), buf(k, "spread"))

    def tables():
        net.arrived(("m", "u", 4))
        net.arrived(("m", "d", 3))
        shape = (2 * toks, 2 * toks)
        row = lax.broadcasted_iota(jnp.int32, shape, 0)
        lane = lax.broadcasted_iota(jnp.int32, shape, 1)
        expert = z * PLANE + lax.rem(p + row // 16, PLANE)
        target = (expert * CAP + lax.rem(row, CAP)).astype(f32)
        second = lane >= toks
        valid = (lax.rem(row // CAP, 2) == 1) == second
        low = lax.broadcasted_iota(jnp.int32, (16, 2 * toks), 1) < toks
        for xi in range(meta_width):
            for i in range(NZ // 2):
                both = jnp.where(low, meta[2 * i, xi], meta[2 * i + 1, xi])
                chosen = jnp.zeros(shape, f32)
                weighted = jnp.zeros(shape, f32)
                for r in range(4):
                    hit = (both[r : r + 1, :] == target) & valid
                    chosen = jnp.where(hit, 1.0, chosen)
                    weighted = jnp.where(hit, both[8 + r : 9 + r, :], weighted)
                pick[xi, i] = chosen.astype(bf16)
                mixed = weighted.T
                high = mixed.astype(bf16)
                mix_hi[xi, i] = high
                mix_lo[xi, i] = (mixed - high.astype(f32)).astype(bf16)

    def select(k):
        net.arrived((k, "u", up_hops(k)))
        net.arrived((k, "d", 7 - up_hops(k)))
        spread, chosen = buf(k, "spread"), buf(k, "chosen")
        for xi in range(place[k][2]):
            for i in range(NZ // 2):
                pair = jnp.concatenate([spread[2 * i, xi], spread[2 * i + 1, xi]], axis=0)
                got = jnp.dot(pick[xi, i], pair, preferred_element_type=f32).astype(bf16)
                rows[k, xi, 16 * i : 16 * i + 16, :] = got[0:16]
                for q in range(1, PLANE):
                    chosen[q, xi, 16 * i : 16 * i + 16, :] = got[16 * q : 16 * q + 16]
        for q in range(1, PLANE):
            net.send(
                (k, "y", q), chosen.at[q],
                rows.at[k, pl.ds(0, place[k][2]), pl.ds(q * toks, toks), :], ahead[q],
            )

    def gather_rows(k):
        first, second = pl.ds(0, half), pl.ds(half, half)
        for q in range(1, PLANE // 2):
            net.arrived((k, "y", q))
        net.send((k, "rA"), rows.at[k, 0, first, :], rows.at[k, 1, first, :], right)
        for q in range(PLANE // 2, PLANE):
            net.arrived((k, "y", q))
        net.send((k, "lB"), rows.at[k, 0, second, :], rows.at[k, 2, second, :], left)
        net.send((k, "rB"), rows.at[k, 0, second, :], rows.at[k, 1, second, :], right)
        net.send((k, "lA"), rows.at[k, 0, first, :], rows.at[k, 2, first, :], left)

    def forward_rows(k):
        first, second = pl.ds(0, half), pl.ds(half, half)
        net.arrived((k, "rA"))
        net.send((k, "fA"), rows.at[k, 1, first, :], rows.at[k, 3, first, :], right)
        net.arrived((k, "lB"))
        net.send((k, "fB"), rows.at[k, 2, second, :], rows.at[k, 3, second, :], left)

    def expert_in(k, first, last):
        if k in WIDE:
            for q in range(1, PLANE):
                net.arrived((k, "y", q))
        else:
            for name in ("rB", "lA", "fA", "fB"):
                net.arrived((k, name))
        if first:
            weight_copies[0].wait()
            weight_copies[1].wait()

        def tile(i, _):
            xi, part = i // 2, lax.rem(i, 2)
            a = rows[k, xi, pl.ds(pl.multiple_of(part * half, half), half), :]
            at = pl.ds(pl.multiple_of(i * half, half), half)
            g = jnp.dot(a, wg[cols(k), :], preferred_element_type=f32)
            u = jnp.dot(a, wu[cols(k), :], preferred_element_type=f32)
            if not first:
                g = g + gate_acc[at, :]
                u = u + up_acc[at, :]
            if last:
                c = jnp.minimum(g, swiglu_limit)
                u = jnp.clip(u, -swiglu_limit, swiglu_limit)
                hidden[at, :] = ((u + 1.0) * c * jax.nn.sigmoid(swiglu_alpha * c)).astype(bf16)
            else:
                gate_acc[at, :] = g
                up_acc[at, :] = u
            return 0

        lax.fori_loop(0, 2 * NX, tile, 0)

    def expert_out(k, first):
        if first:
            weight_copies[2].wait()
        for q in range(1, PLANE):
            net.sent((k, "y", q))
        if k not in WIDE:
            for name in ("rA", "lB", "rB", "lA", "fA", "fB"):
                net.sent((k, name))

        def tile(i, _):
            xi, part = i // 2, lax.rem(i, 2)
            at = pl.ds(pl.multiple_of(i * half, half), half)
            made = jnp.dot(hidden[at, :], wd[:, cols(k)], preferred_element_type=f32)
            rows[k, xi, pl.ds(pl.multiple_of(part * half, half), half), :] = made.astype(bf16)
            return 0

        lax.fori_loop(0, 2 * NX, tile, 0)
        a, b = pl.ds(0, half), pl.ds(half, half)
        if k in WIDE:
            back = buf(k, "back")
            for q in range(1, PLANE):
                net.send((k, "b", q), rows.at[k, pl.ds(0, NX), pl.ds(q * toks, toks), :], back.at[q], behind[q])
        else:
            net.send((k, "oA"), rows.at[k, 3, a, :], buf(k, "hop_r"), right)
            net.send((k, "oB"), rows.at[k, 3, b, :], buf(k, "hop_l"), left)
            net.send((k, "dB"), rows.at[k, 2, b, :], buf(k, "sum_r").at[b, :], right)
            net.send((k, "dA"), rows.at[k, 1, a, :], buf(k, "sum_l").at[a, :], left)

    def reduce_hop(k):
        a, b = pl.ds(0, half), pl.ds(half, half)
        net.arrived((k, "oA"))
        rows[k, 2, a, :] = (rows[k, 2, a, :].astype(f32) + buf(k, "hop_r")[...].astype(f32)).astype(bf16)
        net.send((k, "sA"), rows.at[k, 2, a, :], buf(k, "sum_r").at[a, :], right)
        net.arrived((k, "oB"))
        rows[k, 1, b, :] = (rows[k, 1, b, :].astype(f32) + buf(k, "hop_l")[...].astype(f32)).astype(bf16)
        net.send((k, "sB"), rows.at[k, 1, b, :], buf(k, "sum_l").at[b, :], left)

    def reduce_rows(k):
        for name in ("dB", "dA", "sA", "sB"):
            net.arrived((k, name))
        back, total = buf(k, "back"), buf(k, "total")
        total[...] = (
            rows[k, 0].astype(f32) + buf(k, "sum_r")[...].astype(f32) + buf(k, "sum_l")[...].astype(f32)
        ).astype(bf16)
        for q in range(1, PLANE):
            net.send((k, "b", q), total.at[pl.ds(q * toks, toks), :], back.at[q, 0], behind[q])

    def combine(k):
        for q in range(1, PLANE):
            net.arrived((k, "b", q))
        back, mixed = buf(k, "back"), buf(k, "mixed")
        for xi in range(place[k][2]):
            for i in range(NZ // 2):
                part = slice(16 * i, 16 * i + 16)
                own = rows[k, xi, part, :] if k in WIDE else buf(k, "total")[part, :]
                outs = jnp.concatenate([own] + [back[q, xi, part, :] for q in range(1, PLANE)], axis=0)
                got = jnp.dot(mix_hi[xi, i], outs, preferred_element_type=f32)
                got = got + jnp.dot(mix_lo[xi, i], outs, preferred_element_type=f32)
                mixed[2 * i, xi] = got[:toks]
                mixed[2 * i + 1, xi] = got[toks:]

    def return_hop(k, h):
        mixed, leaving = buf(k, "mixed"), buf(k, "leaving")
        for way, hops, slot, landing, to in (
            ("D", up_hops(k), up_slot, buf(k, "from_up"), down),
            ("U", 7 - up_hops(k), down_slot, buf(k, "from_down"), up),
        ):
            j = hops - h + 1
            if j < 1:
                continue
            value = mixed[slot(j)]
            if h > 1:
                net.arrived((k, way, h - 1))
                value = value + landing[j].astype(f32)
            leaving[slot(j)] = value.astype(bf16)
            net.send((k, way, h), leaving.at[slot(j)], landing.at[j - 1], to)

    def finish(k):
        mixed = buf(k, "mixed")
        net.arrived((k, "D", up_hops(k)))
        net.arrived((k, "U", 7 - up_hops(k)))
        value = mixed[0] + buf(k, "from_up")[0].astype(f32) + buf(k, "from_down")[0].astype(f32)
        if k in WIDE:
            mixed[0] = value
            leaving = buf(k, "leaving")
            leaving[0] = value.astype(bf16)
            last = buf(k, "last")
            net.send((k, "X", 2), leaving.at[0, 2], last.at[2], right)
            net.send((k, "X", 1), leaving.at[0, 1], last.at[1], left)
            net.send((k, "X", 3), leaving.at[0, 3], last.at[3], far)
        else:
            out_ref[:, cols(k)] = (mid_ref[:, cols(k)].astype(f32) + value[0]).astype(bf16)

    def finish_wide(k):
        mixed, last = buf(k, "mixed"), buf(k, "last")
        value = mixed[0, 0]
        for i in (1, 2, 3):
            net.arrived((k, "X", i))
            value = value + last[i].astype(f32)
        out_ref[:, cols(k)] = (mid_ref[:, cols(k)].astype(f32) + value).astype(bf16)

    def run(steps):
        for _, _, step, args in sorted(steps, key=lambda s: s[:2]):
            step(*args)

    meta_first()
    for k in WIDE:
        wide_first(k)
    for k in range(CHUNKS):
        own_tokens(k)
    for h in range(1, 2):
        meta_hop(h)
    order = narrow + list(WIDE)
    steps = []
    for h in range(2, 5):
        steps.append((h - 1, 0, meta_hop, (h,)))
    steps.append((4, 4.5, tables, ()))
    for t, k in enumerate(order):
        for h in range(1, 5):
            steps.append((t + h - 1, 5 - h, token_hop, (k, h)))
        steps.append((t + 4, 5, select, (k,)))
        if k not in WIDE:
            steps.append((t + 5, 6, gather_rows, (k,)))
            steps.append((t + 7, 7, forward_rows, (k,)))
        steps.append((t + 9, 8, expert_in, (k, t == 0, t == CHUNKS - 1)))
    run(steps)

    order = list(WIDE) + narrow
    steps = []
    for t, k in enumerate(order):
        steps.append((t, 5, expert_out, (k, t == 0)))
        if k not in WIDE:
            steps.append((t + 1, 6, reduce_hop, (k,)))
            steps.append((t + 3, 7, reduce_rows, (k,)))
        steps.append((t + 4, 8, combine, (k,)))
        for h in range(1, 5):
            steps.append((t + 4 + h, 5 - h, return_hop, (k, h)))
        steps.append((t + 9, 0, finish, (k,)))
        if k in WIDE:
            steps.append((t + 11, 0.5, finish_wide, (k,)))
    run(steps)
    for name in net.copies:
        net.sent(name)
    assert net.used == sems.shape[0], net.used


def moe(tokens, meta, middle, w_gate, w_up, w_down):
    bf16, f32 = jnp.bfloat16, jnp.float32
    toks, model = tokens.shape
    width = model // CHUNKS
    units = w_gate.shape[2]
    block = PLANE * toks
    wides = len(WIDE)
    meta_width = NX if WIDE else 1

    def group(count, nx):
        if count == 0:
            return {"none": pltpu.VMEM((16, 128), bf16)}
        shapes = {
            "spread": pltpu.VMEM((count, NZ, nx, toks, width), bf16),
            "chosen": pltpu.VMEM((count, PLANE, nx, toks, width), bf16),
            "back": pltpu.VMEM((count, PLANE, nx, toks, width), bf16),
            "mixed": pltpu.VMEM((count, NZ, nx, toks, width), f32),
            "leaving": pltpu.VMEM((count, NZ, nx, toks, width), bf16),
            "from_up": pltpu.VMEM((count, 4, nx, toks, width), bf16),
            "from_down": pltpu.VMEM((count, 4, nx, toks, width), bf16),
        }
        if nx == 1:
            shapes["hop_r"] = pltpu.VMEM((count, block // 2, width), bf16)
            shapes["hop_l"] = pltpu.VMEM((count, block // 2, width), bf16)
            shapes["sum_r"] = pltpu.VMEM((count, block, width), bf16)
            shapes["sum_l"] = pltpu.VMEM((count, block, width), bf16)
            shapes["total"] = pltpu.VMEM((count, block, width), bf16)
        else:
            shapes["last"] = pltpu.VMEM((count, nx, toks, width), bf16)
        return shapes

    per_narrow = 7 + 7 + 6 + 6 + 7 + 7
    per_wide = 3 + 7 + 7 + 7 + 7 + 3
    copies = 7 + (3 if WIDE else 0) + (CHUNKS - wides) * per_narrow + wides * per_wide
    any_spec = pl.BlockSpec(memory_space=pl.ANY)
    vmem_spec = pl.BlockSpec(memory_space=pltpu.VMEM)
    narrow_shapes, wide_shapes = group(CHUNKS - wides, 1), group(wides, NX)
    names_n, names_w = list(narrow_shapes), list(wide_shapes)

    def body(*refs):
        fixed, rest = refs[:18], refs[18:]
        scr_n = dict(zip(names_n, rest[: len(names_n)]))
        rest = rest[len(names_n) :]
        scr_w = dict(zip(names_w, rest[: len(names_w)]))
        sems, wsem = rest[len(names_w) :]
        moe_kernel(*fixed, scr_n, scr_w, sems, wsem)

    tables = [pltpu.VMEM((meta_width, NZ // 2, 2 * toks, 2 * toks), bf16) for _ in range(3)]
    return pl.pallas_call(
        body,
        out_shape=jax.ShapeDtypeStruct((toks, model), bf16),
        in_specs=[vmem_spec, vmem_spec, vmem_spec, any_spec, any_spec, any_spec],
        out_specs=vmem_spec,
        scratch_shapes=[
            pltpu.VMEM((model, units), bf16),
            pltpu.VMEM((model, units), bf16),
            pltpu.VMEM((units, model), bf16),
            pltpu.VMEM((CHUNKS, NX, block, width), bf16),
            pltpu.VMEM((NX * block, units), f32),
            pltpu.VMEM((NX * block, units), f32),
            pltpu.VMEM((NX * block, units), bf16),
            pltpu.VMEM((NZ, meta_width, 16, 2 * toks), f32),
            *tables,
            *narrow_shapes.values(),
            *wide_shapes.values(),
            pltpu.SemaphoreType.DMA((2 * copies,)),
            pltpu.SemaphoreType.DMA((3,)),
        ],
        compiler_params=pltpu.CompilerParams(
            collective_id=0, has_side_effects=True, vmem_limit_bytes=VMEM_LIMIT
        ),
        name="experts",
    )(tokens, meta, middle, w_gate, w_up, w_down)


def route_table(own_routes, weights):
    routes = own_routes.T
    top, toks = routes.shape
    ids = jnp.arange(toks, dtype=jnp.int32)
    same = routes[:, :, None, None] == routes[None, None, :, :]
    earlier = ids[None, None, None, :] < ids[None, :, None, None]
    rank = jnp.sum((same & earlier).astype(jnp.int32), axis=(2, 3))
    slots = (routes * CAP + rank).astype(jnp.float32)
    pad = jnp.full((8 - top, toks), -1.0, jnp.float32)
    table = jnp.concatenate([slots, pad, weights.T, pad], axis=0)
    return jnp.concatenate([table, table], axis=1)


def per_device(
    resid,
    queries,
    keys,
    values,
    docs,
    q_gain,
    key_norm_gain,
    sink,
    out_gain,
    w_out,
    norm_gain,
    routes,
    route_weights,
    w_gate,
    w_up,
    w_down,
):
    tp_size = lax.axis_size("tp")
    sp_index = lax.axis_index("sp")
    tp_index = lax.axis_index("tp")
    tok_rows = queries.shape[0]
    head_size = q_gain.shape[0]
    query_heads = sink.shape[0]
    kv_heads = keys.shape[1] // head_size
    query_group_width = query_heads // kv_heads
    token_positions = (sp_index * tok_rows + jnp.arange(tok_rows, dtype=jnp.int32)).astype(
        jnp.float32
    )
    q_rot = apply_rotary_heads(
        row_normalize(queries.reshape(tok_rows, query_heads, head_size), q_gain), token_positions
    ).astype(jnp.bfloat16)
    key_rotated = apply_rotary_heads(
        row_normalize(keys.reshape(tok_rows, kv_heads, head_size), key_norm_gain), token_positions
    ).astype(jnp.bfloat16)
    key_value = jnp.concatenate(
        [key_rotated.reshape(tok_rows, kv_heads * head_size), values], axis=1
    )
    doc_mark = (docs + 1).astype(jnp.bfloat16)
    kv_span, doc_span = (
        extended(key_value, (("sp", 0),), WINDOW),
        extended(doc_mark, (("sp", 0),), WINDOW),
    )
    span_rows = tok_rows + 2 * WINDOW
    k_span = kv_span[:, : kv_heads * head_size].reshape(span_rows, kv_heads, head_size)
    v_span = kv_span[:, kv_heads * head_size :].reshape(span_rows, kv_heads, head_size)
    scores = jnp.einsum(
        "qhgd,khd->hgqk",
        q_rot.reshape(tok_rows, kv_heads, query_group_width, head_size),
        k_span,
        preferred_element_type=jnp.float32,
    ) * head_size ** (-0.5)
    offsets = jnp.arange(tok_rows, dtype=jnp.int32)[:, None] - (
        jnp.arange(span_rows, dtype=jnp.int32)[None, :] - WINDOW
    )
    allowed = (jnp.abs(offsets) <= WINDOW) & (doc_mark[:, None] == doc_span[None, :])
    raw_weights = jnp.where(allowed[None, None], jnp.exp(scores), jnp.zeros((), jnp.float32))
    sink_exponent = jnp.exp(sink).reshape(kv_heads, query_group_width)
    total = jnp.sum(raw_weights, axis=-1) + sink_exponent[:, :, None]
    probs = (raw_weights / total[..., None]).astype(jnp.bfloat16)
    att = jnp.einsum("hgqk,khd->qhgd", probs, v_span, preferred_element_type=jnp.float32)
    att = att.astype(jnp.bfloat16).reshape(tok_rows, query_heads * head_size)
    by_token = lax.all_to_all(att, "tp", split_axis=0, concat_axis=1, tiled=True)
    att_normed = row_normalize(by_token, out_gain).astype(jnp.bfloat16)
    middle = (
        resid.astype(jnp.float32) + jnp.dot(att_normed, w_out, preferred_element_type=jnp.float32)
    ).astype(jnp.bfloat16)
    moe_in = row_normalize(middle, norm_gain).astype(jnp.bfloat16)
    quarter = tok_rows // tp_size
    own_routes = lax.dynamic_slice_in_dim(routes, tp_index * quarter, quarter, 0)
    table = route_table(own_routes, route_weights)
    return moe(moe_in, table, middle, w_gate, w_up, w_down)


def solution(mesh):
    return jax.shard_map(
        per_device,
        mesh=mesh,
        in_specs=(
            P(("sp", "tp"), None),
            P("sp", "tp"),
            P("sp", "tp"),
            P("sp", "tp"),
            P("sp"),
            P(),
            P(),
            P("tp"),
            P(),
            P(),
            P(),
            P("sp", None),
            P(("sp", "tp"), None),
            P("sp", None, "tp"),
            P("sp", None, "tp"),
            P("sp", "tp", None),
        ),
        out_specs=P(("sp", "tp"), None),
        check_vma=False,
    )
```

```python
import jax
import jax.numpy as jnp
from jax import lax
from jax.experimental import pallas as pl
from jax.experimental.pallas import tpu as pltpu
from jax.sharding import PartitionSpec as P

WINDOW = 128
MESH = pl.DeviceIdType.MESH

NZ = 8
PLANE = 8
NX = 4
CAP = 8
CHUNKS = 8
WIDE = (6, 7)
VMEM_LIMIT = 63 * 1024 * 1024
ORDER = (
    (0,), (1, 1), (5, 1, 1), (5, 0, 1), (4, 6), (1, 2), (5, 1, 2), (5, 4, 1), (1, 3), (5, 1, 3), (5, 0, 2), (1, 4),
    (5, 1, 4), (5, 4, 2), (4, 7), (5, 0, 3), (3, 0), (6, 1), (5, 3, 1), (5, 5, 1), (5, 2, 1), (5, 0, 4), (5, 4, 3),
    (5, 3, 2), (5, 5, 2), (5, 2, 2), (7, 1), (5, 4, 4), (6, 0), (5, 7, 1), (5, 3, 3), (5, 2, 3), (8, 1), (6, 4),
    (2, 1), (5, 5, 3), (7, 0), (5, 3, 4), (5, 7, 2), (6, 3), (2, 2), (7, 4), (5, 2, 4), (5, 5, 4), (8, 0),
    (5, 7, 3), (8, 4), (6, 2), (6, 5), (2, 3), (5, 6, 1), (7, 3), (5, 7, 4), (2, 4), (7, 2), (5, 6, 2), (3, 1),
    (6, 7), (5, 6, 3), (5, 6, 4), (7, 5), (9, 1), (8, 3), (9, 4), (6, 6), (9, 7), (8, 2), (8, 5), (9, 0), (9, 3),
    (9, 2), (9, 5), (9, 6), (10, 6), (10, 7), (10, 0), (10, 1), (11, 1), (11, 0), (10, 2), (13, 6), (14, 6, 1),
    (10, 3), (14, 6, 2), (12, 1), (13, 7), (12, 0), (14, 7, 1), (14, 6, 3), (14, 7, 2), (11, 2), (11, 3), (10, 4),
    (12, 2), (13, 1), (14, 1, 1), (14, 7, 3), (14, 1, 2), (13, 0), (14, 6, 4), (11, 4), (14, 0, 1), (12, 3),
    (10, 5), (13, 2), (14, 2, 1), (14, 1, 3), (14, 7, 4), (12, 4), (14, 1, 4), (14, 0, 2), (11, 5), (14, 2, 2),
    (15, 7), (13, 3), (14, 3, 1), (15, 1), (14, 2, 3), (13, 4), (12, 5), (14, 4, 1), (14, 3, 2), (15, 6),
    (14, 0, 3), (14, 3, 3), (14, 4, 2), (13, 5), (14, 5, 1), (14, 4, 3), (14, 5, 2), (14, 0, 4), (14, 5, 3),
    (14, 4, 4), (14, 2, 4), (14, 3, 4), (15, 0), (14, 5, 4), (16, 6), (16, 7), (15, 4), (15, 3), (15, 2), (15, 5),
)


rope_base = 10000.0
norm_eps = 1e-06
swiglu_limit = 7.0
swiglu_alpha = 1.702


def extended(x, sides, width):
    for axis, dim in sides:
        peers, length = (lax.axis_size(axis), x.shape[dim])
        up = [(i, (i + 1) % peers) for i in range(peers - 1)]
        down = [(j, i) for i, j in up]
        last = lax.slice_in_dim(x, length - width, length, axis=dim)
        leading = lax.slice_in_dim(x, 0, width, axis=dim)
        before = lax.ppermute(last, axis, up)
        after = lax.ppermute(leading, axis, down)
        x = jnp.concatenate([before, x, after], axis=dim)
    return x


def row_normalize(values, gain_vec):
    floats = values.astype(jnp.float32)
    scale_inv = lax.rsqrt(jnp.mean(floats * floats, axis=-1, keepdims=True) + norm_eps)
    return floats * scale_inv * gain_vec


def apply_rotary_heads(heads, token_positions):
    half_size = heads.shape[-1] // 2
    freqs = rope_base ** (-jnp.arange(half_size, dtype=jnp.float32) / half_size)
    angles = token_positions[:, None] * freqs[None, :]
    cosine = jnp.cos(angles)[:, None, :]
    sine = jnp.sin(angles)[:, None, :]
    first_half = heads[..., :half_size]
    second_half = heads[..., half_size:]
    return jnp.concatenate(
        [first_half * cosine - second_half * sine, first_half * sine + second_half * cosine],
        axis=-1,
    )


class Net:
    def __init__(self, sems):
        self.sems = sems
        self.used = 0
        self.copies = {}

    def send(self, name, src, dst, device):
        copy = pltpu.make_async_remote_copy(
            src_ref=src,
            dst_ref=dst,
            send_sem=self.sems.at[self.used],
            recv_sem=self.sems.at[self.used + 1],
            device_id=device,
            device_id_type=MESH,
        )
        self.used += 2
        copy.start()
        self.copies[name] = [copy, False]

    def arrived(self, name):
        self.copies[name][0].wait_recv()

    def sent(self, name):
        if not self.copies[name][1]:
            self.copies[name][0].wait_send()
            self.copies[name][1] = True


def moe_kernel(
    tok_ref, meta_ref, mid_ref, wg_hbm, wu_hbm, wd_hbm, out_ref,
    wg, wu, wd, rows, gate_acc, up_acc, hidden, meta, pick, mix_hi, mix_lo,
    scr_narrow, scr_wide, sems, wsem,
):
    bf16, f32 = jnp.bfloat16, jnp.float32
    width = tok_ref.shape[1] // CHUNKS
    toks = tok_ref.shape[0]
    block = PLANE * toks
    half = block // 2
    sp, x = lax.axis_index("sp"), lax.axis_index("tp")
    z, p = sp // PLANE, lax.rem(sp, PLANE)
    z_up = lax.rem(z + 1, NZ) * PLANE + p
    z_down = lax.rem(z + NZ - 1, NZ) * PLANE + p
    x_up, x_down, x_far = lax.rem(x + 1, NX), lax.rem(x + NX - 1, NX), lax.rem(x + 2, NX)
    up, down = (z_up, x), (z_down, x)
    right, left, far = (sp, x_up), (sp, x_down), (sp, x_far)
    ahead = [(z * PLANE + lax.rem(p + q, PLANE), x) for q in range(PLANE)]
    behind = [(z * PLANE + lax.rem(p + PLANE - q, PLANE), x) for q in range(PLANE)]
    net = Net(sems)
    narrow = [k for k in range(CHUNKS) if k not in WIDE]
    place = {k: (scr_wide, WIDE.index(k), NX) if k in WIDE else (scr_narrow, narrow.index(k), 1) for k in range(CHUNKS)}

    def buf(k, name):
        group, i, _ = place[k]
        return group[name].at[i]

    def cols(k):
        return slice(k * width, (k + 1) * width)

    weight_copies = [
        pltpu.make_async_copy(src.at[0], dst, wsem.at[i])
        for i, (src, dst) in enumerate(((wg_hbm, wg), (wu_hbm, wu), (wd_hbm, wd)))
    ]
    for copy in weight_copies:
        copy.start()

    meta[0, 0] = meta_ref[...]
    for k in range(CHUNKS):
        buf(k, "spread")[0, 0] = tok_ref[:, cols(k)]

    barrier = pltpu.get_barrier_semaphore()
    peers = [up, down, right, left] + ahead[1:] + ([far] if WIDE else [])
    for peer in peers:
        pl.semaphore_signal(barrier, inc=1, device_id=peer, device_id_type=MESH)
    pl.semaphore_wait(barrier, len(peers))

    meta_width = NX if WIDE else 1

    def up_hops(k):
        return 4 if k % 2 == 0 else 3

    def up_slot(h):
        return h

    def down_slot(h):
        return 4 if h == 4 else (0 if h == 0 else 4 + h)

    def wide_first(k):
        spread = buf(k, "spread")
        src = tok_ref.at[:, cols(k)]
        net.send((k, "w", 1), src, spread.at[0, 1], right)
        net.send((k, "w", 2), src, spread.at[0, 2], left)
        net.send((k, "w", 3), src, spread.at[0, 3], far)

    def meta_first():
        if WIDE:
            net.send(("mw", 1), meta_ref, meta.at[0, 1], right)
            net.send(("mw", 2), meta_ref, meta.at[0, 2], left)
            net.send(("mw", 3), meta_ref, meta.at[0, 3], far)

    def ring_hop(name, h, last_up, last_down, data):
        if h <= last_up:
            if h > 1:
                net.arrived((name, "u", h - 1))
            net.send((name, "u", h), data.at[up_slot(h - 1)], data.at[up_slot(h)], up)
        if h <= last_down:
            if h > 1:
                net.arrived((name, "d", h - 1))
            net.send((name, "d", h), data.at[down_slot(h - 1)], data.at[down_slot(h)], down)

    def meta_hop(h):
        ring_hop("m", h, 4, 3, meta.at[:, 0])

    def meta_wide_hop(h):
        if h == 1:
            for i in (1, 2, 3):
                net.arrived(("mw", i))
        ring_hop("mz", h, 4, 3, meta.at[:, pl.ds(1, NX - 1)])

    def token_hop(k, h):
        if h == 1 and k in WIDE:
            for i in (1, 2, 3):
                net.arrived((k, "w", i))
        ring_hop(k, h, up_hops(k), 7 - up_hops(k), buf(k, "spread"))

    def tables(others):
        indices = range(1, NX) if others else (0,)
        net.arrived(("mz" if others else "m", "u", 4))
        net.arrived(("mz" if others else "m", "d", 3))
        shape = (2 * toks, 2 * toks)
        row = lax.broadcasted_iota(jnp.int32, shape, 0)
        lane = lax.broadcasted_iota(jnp.int32, shape, 1)
        expert = z * PLANE + lax.rem(p + row // 16, PLANE)
        target = (expert * CAP + lax.rem(row, CAP)).astype(f32)
        second = lane >= toks
        valid = (lax.rem(row // CAP, 2) == 1) == second
        low = lax.broadcasted_iota(jnp.int32, (16, 2 * toks), 1) < toks
        for xi in indices:
            for i in range(NZ // 2):
                both = jnp.where(low, meta[2 * i, xi], meta[2 * i + 1, xi])
                chosen = jnp.zeros(shape, f32)
                weighted = jnp.zeros(shape, f32)
                for r in range(4):
                    hit = (both[r : r + 1, :] == target) & valid
                    chosen = jnp.where(hit, 1.0, chosen)
                    weighted = jnp.where(hit, both[8 + r : 9 + r, :], weighted)
                pick[xi, i] = chosen.astype(bf16)
                mixed = weighted.T
                high = mixed.astype(bf16)
                mix_hi[xi, i] = high
                mix_lo[xi, i] = (mixed - high.astype(f32)).astype(bf16)

    def select(k):
        net.arrived((k, "u", up_hops(k)))
        net.arrived((k, "d", 7 - up_hops(k)))
        spread, chosen = buf(k, "spread"), buf(k, "chosen")
        for xi in range(place[k][2]):
            for i in range(NZ // 2):
                pair = jnp.concatenate([spread[2 * i, xi], spread[2 * i + 1, xi]], axis=0)
                got = jnp.dot(pick[xi, i], pair, preferred_element_type=f32).astype(bf16)
                rows[k, xi, 16 * i : 16 * i + 16, :] = got[0:16]
                for q in range(1, PLANE):
                    chosen[q, xi, 16 * i : 16 * i + 16, :] = got[16 * q : 16 * q + 16]
        for q in (4, 5, 2, 3, 6, 7, 1):
            net.send(
                (k, "y", q), chosen.at[q],
                rows.at[k, pl.ds(0, place[k][2]), pl.ds(q * toks, toks), :], ahead[q],
            )

    def gather_rows(k):
        first, second = pl.ds(0, half), pl.ds(half, half)
        for q in range(1, PLANE // 2):
            net.arrived((k, "y", q))
        net.send((k, "rA"), rows.at[k, 0, first, :], rows.at[k, 1, first, :], right)
        for q in range(PLANE // 2, PLANE):
            net.arrived((k, "y", q))
        net.send((k, "lB"), rows.at[k, 0, second, :], rows.at[k, 2, second, :], left)
        net.send((k, "rB"), rows.at[k, 0, second, :], rows.at[k, 1, second, :], right)
        net.send((k, "lA"), rows.at[k, 0, first, :], rows.at[k, 2, first, :], left)

    def forward_rows(k):
        first, second = pl.ds(0, half), pl.ds(half, half)
        net.arrived((k, "rA"))
        net.send((k, "fA"), rows.at[k, 1, first, :], rows.at[k, 3, first, :], right)
        net.arrived((k, "lB"))
        net.send((k, "fB"), rows.at[k, 2, second, :], rows.at[k, 3, second, :], left)

    def expert_in(k, first, last):
        if k in WIDE:
            for q in range(1, PLANE):
                net.arrived((k, "y", q))
        else:
            for name in ("rB", "lA", "fA", "fB"):
                net.arrived((k, name))
        if first:
            weight_copies[0].wait()
            weight_copies[1].wait()

        def tile(i, _):
            xi, part = i // 2, lax.rem(i, 2)
            a = rows[k, xi, pl.ds(pl.multiple_of(part * half, half), half), :]
            at = pl.ds(pl.multiple_of(i * half, half), half)
            g = jnp.dot(a, wg[cols(k), :], preferred_element_type=f32)
            u = jnp.dot(a, wu[cols(k), :], preferred_element_type=f32)
            if not first:
                g = g + gate_acc[at, :]
                u = u + up_acc[at, :]
            if last:
                c = jnp.minimum(g, swiglu_limit)
                u = jnp.clip(u, -swiglu_limit, swiglu_limit)
                hidden[at, :] = ((u + 1.0) * c * jax.nn.sigmoid(swiglu_alpha * c)).astype(bf16)
            else:
                gate_acc[at, :] = g
                up_acc[at, :] = u
            return 0

        lax.fori_loop(0, 2 * NX, tile, 0)

    def expert_out(k, first):
        if first:
            weight_copies[2].wait()
        for q in range(1, PLANE):
            net.sent((k, "y", q))
        if k not in WIDE:
            for name in ("rA", "lB", "rB", "lA", "fA", "fB"):
                net.sent((k, name))

        def tile(i, _):
            xi, part = i // 2, lax.rem(i, 2)
            at = pl.ds(pl.multiple_of(i * half, half), half)
            made = jnp.dot(hidden[at, :], wd[:, cols(k)], preferred_element_type=f32)
            rows[k, xi, pl.ds(pl.multiple_of(part * half, half), half), :] = made.astype(bf16)
            return 0

        lax.fori_loop(0, 2 * NX, tile, 0)
        a, b = pl.ds(0, half), pl.ds(half, half)
        if k in WIDE:
            back = buf(k, "back")
            for q in (4, 5, 2, 3, 6, 7, 1):
                net.send((k, "b", q), rows.at[k, pl.ds(0, NX), pl.ds(q * toks, toks), :], back.at[q], behind[q])
        else:
            net.send((k, "oA"), rows.at[k, 3, a, :], buf(k, "hop_r"), right)
            net.send((k, "oB"), rows.at[k, 3, b, :], buf(k, "hop_l"), left)
            net.send((k, "dB"), rows.at[k, 2, b, :], buf(k, "sum_r").at[b, :], right)
            net.send((k, "dA"), rows.at[k, 1, a, :], buf(k, "sum_l").at[a, :], left)

    def reduce_hop(k):
        a, b = pl.ds(0, half), pl.ds(half, half)
        net.arrived((k, "oA"))
        rows[k, 2, a, :] = (rows[k, 2, a, :].astype(f32) + buf(k, "hop_r")[...].astype(f32)).astype(bf16)
        net.send((k, "sA"), rows.at[k, 2, a, :], buf(k, "sum_r").at[a, :], right)
        net.arrived((k, "oB"))
        rows[k, 1, b, :] = (rows[k, 1, b, :].astype(f32) + buf(k, "hop_l")[...].astype(f32)).astype(bf16)
        net.send((k, "sB"), rows.at[k, 1, b, :], buf(k, "sum_l").at[b, :], left)

    def reduce_rows(k):
        for name in ("dB", "dA", "sA", "sB"):
            net.arrived((k, name))
        back, total = buf(k, "back"), buf(k, "total")
        total[...] = (
            rows[k, 0].astype(f32) + buf(k, "sum_r")[...].astype(f32) + buf(k, "sum_l")[...].astype(f32)
        ).astype(bf16)
        for q in (4, 5, 2, 3, 6, 7, 1):
            net.send((k, "b", q), total.at[pl.ds(q * toks, toks), :], back.at[q, 0], behind[q])

    def combine(k):
        for q in range(1, PLANE):
            net.arrived((k, "b", q))
        back, mixed = buf(k, "back"), buf(k, "mixed")
        for xi in range(place[k][2]):
            for i in range(NZ // 2):
                part = slice(16 * i, 16 * i + 16)
                own = rows[k, xi, part, :] if k in WIDE else buf(k, "total")[part, :]
                outs = jnp.concatenate([own] + [back[q, xi, part, :] for q in range(1, PLANE)], axis=0)
                got = jnp.dot(mix_hi[xi, i], outs, preferred_element_type=f32)
                got = got + jnp.dot(mix_lo[xi, i], outs, preferred_element_type=f32)
                mixed[2 * i, xi] = got[:toks]
                mixed[2 * i + 1, xi] = got[toks:]

    def return_hop(k, h):
        mixed, leaving = buf(k, "mixed"), buf(k, "leaving")
        for way, hops, slot, landing, to in (
            ("D", up_hops(k), up_slot, buf(k, "from_up"), down),
            ("U", 7 - up_hops(k), down_slot, buf(k, "from_down"), up),
        ):
            j = hops - h + 1
            if j < 1:
                continue
            value = mixed[slot(j)]
            if h > 1:
                net.arrived((k, way, h - 1))
                value = value + landing[j].astype(f32)
            leaving[slot(j)] = value.astype(bf16)
            net.send((k, way, h), leaving.at[slot(j)], landing.at[j - 1], to)

    def finish(k):
        mixed = buf(k, "mixed")
        net.arrived((k, "D", up_hops(k)))
        net.arrived((k, "U", 7 - up_hops(k)))
        value = mixed[0] + buf(k, "from_up")[0].astype(f32) + buf(k, "from_down")[0].astype(f32)
        if k in WIDE:
            mixed[0] = value
            leaving = buf(k, "leaving")
            leaving[0] = value.astype(bf16)
            last = buf(k, "last")
            net.send((k, "X", 2), leaving.at[0, 2], last.at[2], right)
            net.send((k, "X", 1), leaving.at[0, 1], last.at[1], left)
            net.send((k, "X", 3), leaving.at[0, 3], last.at[3], far)
        else:
            out_ref[:, cols(k)] = (mid_ref[:, cols(k)].astype(f32) + value[0]).astype(bf16)

    def finish_wide(k):
        mixed, last = buf(k, "mixed"), buf(k, "last")
        value = mixed[0, 0]
        for i in (1, 2, 3):
            net.arrived((k, "X", i))
            value = value + last[i].astype(f32)
        out_ref[:, cols(k)] = (mid_ref[:, cols(k)].astype(f32) + value).astype(bf16)

    steps = (
        meta_first, meta_hop, meta_wide_hop, tables, wide_first, token_hop, select, gather_rows, forward_rows,
        expert_in, expert_out, reduce_hop, reduce_rows, combine, return_hop, finish, finish_wide,
    )
    done = {step: 0 for step in steps}
    for number, *args in ORDER:
        step = steps[number]
        if step is expert_in:
            args = args + [done[step] == 0, done[step] == CHUNKS - 1]
        if step is expert_out:
            args = args + [done[step] == 0]
        done[step] += 1
        step(*args)
    for name in net.copies:
        net.sent(name)
    assert net.used == sems.shape[0], net.used


def moe(tokens, meta, middle, w_gate, w_up, w_down):
    bf16, f32 = jnp.bfloat16, jnp.float32
    toks, model = tokens.shape
    width = model // CHUNKS
    units = w_gate.shape[2]
    block = PLANE * toks
    wides = len(WIDE)
    meta_width = NX if WIDE else 1

    def group(count, nx):
        if count == 0:
            return {"none": pltpu.VMEM((16, 128), bf16)}
        shapes = {
            "spread": pltpu.VMEM((count, NZ, nx, toks, width), bf16),
            "chosen": pltpu.VMEM((count, PLANE, nx, toks, width), bf16),
            "back": pltpu.VMEM((count, PLANE, nx, toks, width), bf16),
            "mixed": pltpu.VMEM((count, NZ, nx, toks, width), f32),
            "leaving": pltpu.VMEM((count, NZ, nx, toks, width), bf16),
            "from_up": pltpu.VMEM((count, 4, nx, toks, width), bf16),
            "from_down": pltpu.VMEM((count, 4, nx, toks, width), bf16),
        }
        if nx == 1:
            shapes["hop_r"] = pltpu.VMEM((count, block // 2, width), bf16)
            shapes["hop_l"] = pltpu.VMEM((count, block // 2, width), bf16)
            shapes["sum_r"] = pltpu.VMEM((count, block, width), bf16)
            shapes["sum_l"] = pltpu.VMEM((count, block, width), bf16)
            shapes["total"] = pltpu.VMEM((count, block, width), bf16)
        else:
            shapes["last"] = pltpu.VMEM((count, nx, toks, width), bf16)
        return shapes

    per_narrow = 7 + 7 + 6 + 6 + 7 + 7
    per_wide = 3 + 7 + 7 + 7 + 7 + 3
    copies = 7 + (10 if WIDE else 0) + (CHUNKS - wides) * per_narrow + wides * per_wide
    any_spec = pl.BlockSpec(memory_space=pl.ANY)
    vmem_spec = pl.BlockSpec(memory_space=pltpu.VMEM)
    narrow_shapes, wide_shapes = group(CHUNKS - wides, 1), group(wides, NX)
    names_n, names_w = list(narrow_shapes), list(wide_shapes)

    def body(*refs):
        fixed, rest = refs[:18], refs[18:]
        scr_n = dict(zip(names_n, rest[: len(names_n)]))
        rest = rest[len(names_n) :]
        scr_w = dict(zip(names_w, rest[: len(names_w)]))
        sems, wsem = rest[len(names_w) :]
        moe_kernel(*fixed, scr_n, scr_w, sems, wsem)

    tables = [pltpu.VMEM((meta_width, NZ // 2, 2 * toks, 2 * toks), bf16) for _ in range(3)]
    return pl.pallas_call(
        body,
        out_shape=jax.ShapeDtypeStruct((toks, model), bf16),
        in_specs=[vmem_spec, vmem_spec, vmem_spec, any_spec, any_spec, any_spec],
        out_specs=vmem_spec,
        scratch_shapes=[
            pltpu.VMEM((model, units), bf16),
            pltpu.VMEM((model, units), bf16),
            pltpu.VMEM((units, model), bf16),
            pltpu.VMEM((CHUNKS, NX, block, width), bf16),
            pltpu.VMEM((NX * block, units), f32),
            pltpu.VMEM((NX * block, units), f32),
            pltpu.VMEM((NX * block, units), bf16),
            pltpu.VMEM((NZ, meta_width, 16, 2 * toks), f32),
            *tables,
            *narrow_shapes.values(),
            *wide_shapes.values(),
            pltpu.SemaphoreType.DMA((2 * copies,)),
            pltpu.SemaphoreType.DMA((3,)),
        ],
        compiler_params=pltpu.CompilerParams(
            collective_id=0, has_side_effects=True, vmem_limit_bytes=VMEM_LIMIT
        ),
        name="experts",
    )(tokens, meta, middle, w_gate, w_up, w_down)


def route_table(own_routes, weights):
    routes = own_routes.T
    top, toks = routes.shape
    ids = jnp.arange(toks, dtype=jnp.int32)
    same = routes[:, :, None, None] == routes[None, None, :, :]
    earlier = ids[None, None, None, :] < ids[None, :, None, None]
    rank = jnp.sum((same & earlier).astype(jnp.int32), axis=(2, 3))
    slots = (routes * CAP + rank).astype(jnp.float32)
    pad = jnp.full((8 - top, toks), -1.0, jnp.float32)
    table = jnp.concatenate([slots, pad, weights.T, pad], axis=0)
    return jnp.concatenate([table, table], axis=1)


def per_device(
    resid,
    queries,
    keys,
    values,
    docs,
    q_gain,
    key_norm_gain,
    sink,
    out_gain,
    w_out,
    norm_gain,
    routes,
    route_weights,
    w_gate,
    w_up,
    w_down,
):
    tp_size = lax.axis_size("tp")
    sp_index = lax.axis_index("sp")
    tp_index = lax.axis_index("tp")
    tok_rows = queries.shape[0]
    head_size = q_gain.shape[0]
    query_heads = sink.shape[0]
    kv_heads = keys.shape[1] // head_size
    query_group_width = query_heads // kv_heads
    token_positions = (sp_index * tok_rows + jnp.arange(tok_rows, dtype=jnp.int32)).astype(
        jnp.float32
    )
    q_rot = apply_rotary_heads(
        row_normalize(queries.reshape(tok_rows, query_heads, head_size), q_gain), token_positions
    ).astype(jnp.bfloat16)
    key_rotated = apply_rotary_heads(
        row_normalize(keys.reshape(tok_rows, kv_heads, head_size), key_norm_gain), token_positions
    ).astype(jnp.bfloat16)
    key_value = jnp.concatenate(
        [key_rotated.reshape(tok_rows, kv_heads * head_size), values], axis=1
    )
    doc_mark = (docs + 1).astype(jnp.bfloat16)
    kv_span, doc_span = (
        extended(key_value, (("sp", 0),), WINDOW),
        extended(doc_mark, (("sp", 0),), WINDOW),
    )
    span_rows = tok_rows + 2 * WINDOW
    k_span = kv_span[:, : kv_heads * head_size].reshape(span_rows, kv_heads, head_size)
    v_span = kv_span[:, kv_heads * head_size :].reshape(span_rows, kv_heads, head_size)
    scores = jnp.einsum(
        "qhgd,khd->hgqk",
        q_rot.reshape(tok_rows, kv_heads, query_group_width, head_size),
        k_span,
        preferred_element_type=jnp.float32,
    ) * head_size ** (-0.5)
    offsets = jnp.arange(tok_rows, dtype=jnp.int32)[:, None] - (
        jnp.arange(span_rows, dtype=jnp.int32)[None, :] - WINDOW
    )
    allowed = (jnp.abs(offsets) <= WINDOW) & (doc_mark[:, None] == doc_span[None, :])
    raw_weights = jnp.where(allowed[None, None], jnp.exp(scores), jnp.zeros((), jnp.float32))
    sink_exponent = jnp.exp(sink).reshape(kv_heads, query_group_width)
    total = jnp.sum(raw_weights, axis=-1) + sink_exponent[:, :, None]
    probs = (raw_weights / total[..., None]).astype(jnp.bfloat16)
    att = jnp.einsum("hgqk,khd->qhgd", probs, v_span, preferred_element_type=jnp.float32)
    att = att.astype(jnp.bfloat16).reshape(tok_rows, query_heads * head_size)
    by_token = lax.all_to_all(att, "tp", split_axis=0, concat_axis=1, tiled=True)
    att_normed = row_normalize(by_token, out_gain).astype(jnp.bfloat16)
    middle = (
        resid.astype(jnp.float32) + jnp.dot(att_normed, w_out, preferred_element_type=jnp.float32)
    ).astype(jnp.bfloat16)
    moe_in = row_normalize(middle, norm_gain).astype(jnp.bfloat16)
    quarter = tok_rows // tp_size
    own_routes = lax.dynamic_slice_in_dim(routes, tp_index * quarter, quarter, 0)
    table = route_table(own_routes, route_weights)
    return moe(moe_in, table, middle, w_gate, w_up, w_down)


def solution(mesh):
    return jax.shard_map(
        per_device,
        mesh=mesh,
        in_specs=(
            P(("sp", "tp"), None),
            P("sp", "tp"),
            P("sp", "tp"),
            P("sp", "tp"),
            P("sp"),
            P(),
            P(),
            P("tp"),
            P(),
            P(),
            P(),
            P("sp", None),
            P(("sp", "tp"), None),
            P("sp", None, "tp"),
            P("sp", None, "tp"),
            P("sp", "tp", None),
        ),
        out_specs=P(("sp", "tp"), None),
        check_vma=False,
    )
```

```python
import jax
import jax.numpy as jnp
from jax import lax
from jax.experimental import pallas as pl
from jax.experimental.pallas import tpu as pltpu
from jax.sharding import PartitionSpec as P

WINDOW = 128
MESH = pl.DeviceIdType.MESH

NZ = 8
PLANE = 8
NX = 4
CAP = 8
HEAD = 64
CHUNKS = 8
WIDE = (6, 7)
VMEM_LIMIT = 67_043_328
ORDER = (
    (0,), (1, 1), (5, 1, 1), (5, 0, 1), (4, 7), (1, 2), (4, 6), (5, 1, 2), (5, 3, 1), (1, 3), (5, 1, 3), (5, 0, 2),
    (1, 4), (5, 1, 4), (5, 4, 1), (2, 1), (5, 0, 3), (3, 0), (5, 2, 1), (6, 1), (5, 4, 2), (5, 0, 4), (5, 5, 1),
    (5, 3, 2), (5, 2, 2), (5, 4, 3), (7, 1), (5, 7, 1), (6, 0), (5, 4, 4), (8, 1), (5, 3, 3), (2, 2), (5, 3, 4),
    (5, 5, 2), (7, 0), (5, 7, 2), (5, 2, 3), (6, 4), (2, 3), (6, 3), (8, 0), (5, 5, 3), (5, 2, 4), (7, 4),
    (5, 7, 3), (5, 5, 4), (6, 2), (2, 4), (7, 3), (5, 6, 1), (5, 7, 4), (6, 5), (5, 6, 2), (8, 4), (7, 2), (3, 1),
    (8, 3), (6, 7), (5, 6, 3), (9, 0), (8, 2), (5, 6, 4), (9, 4), (9, 1), (6, 6), (7, 5), (9, 2), (8, 5), (9, 7),
    (9, 3), (9, 5), (9, 6), (10, 6), (10, 7), (10, 0), (10, 1), (11, 1), (11, 0), (10, 2), (10, 3), (13, 6),
    (14, 6, 1), (12, 0), (14, 6, 2), (13, 7), (14, 7, 1), (12, 1), (13, 0), (14, 0, 1), (14, 7, 2), (11, 3),
    (11, 2), (13, 1), (10, 4), (14, 6, 3), (12, 3), (14, 1, 1), (14, 7, 3), (12, 2), (11, 4), (14, 1, 2),
    (14, 0, 2), (14, 6, 4), (10, 5), (14, 7, 4), (13, 2), (14, 2, 1), (12, 4), (13, 3), (14, 3, 1), (14, 1, 3),
    (11, 5), (14, 0, 3), (14, 2, 2), (15, 6), (13, 4), (14, 4, 1), (14, 1, 4), (12, 5), (14, 3, 2), (14, 0, 4),
    (15, 7), (14, 4, 2), (14, 2, 3), (13, 5), (14, 5, 1), (16, 6), (14, 4, 3), (14, 5, 2), (14, 3, 3), (14, 5, 3),
    (14, 4, 4), (14, 2, 4), (15, 1), (15, 0), (14, 3, 4), (14, 5, 4), (15, 4), (15, 3), (16, 7), (15, 2), (15, 5),
)


rope_base = 10000.0
norm_eps = 1e-06
swiglu_limit = 7.0
swiglu_alpha = 1.702


class Net:
    def __init__(self, sems):
        self.sems = sems
        self.used = 0
        self.copies = {}

    def send(self, name, src, dst, device):
        copy = pltpu.make_async_remote_copy(
            src_ref=src,
            dst_ref=dst,
            send_sem=self.sems.at[self.used],
            recv_sem=self.sems.at[self.used + 1],
            device_id=device,
            device_id_type=MESH,
        )
        self.used += 2
        copy.start()
        self.copies[name] = [copy, False]

    def arrived(self, name):
        self.copies[name][0].wait_recv()

    def sent(self, name):
        if not self.copies[name][1]:
            self.copies[name][0].wait_send()
            self.copies[name][1] = True


def moe_kernel(
    q_ref, kv_ref, doc_ref, angle_ref, gain_ref, sink_ref, out_gain_ref, norm_gain_ref, resid_ref, meta_ref,
    wo_hbm, wg_hbm, wu_hbm, wd_hbm, out_ref,
    wo, q_rot, kv_span, doc_span, att, by_token, mid_ref,
    wg, wu, wd, rows, gate_acc, up_acc, hidden, meta, pick, mix_hi, mix_lo,
    scr_narrow, scr_wide, sems, wsem,
):
    bf16, f32 = jnp.bfloat16, jnp.float32
    toks, model = resid_ref.shape
    width = model // CHUNKS
    block = PLANE * toks
    half = block // 2
    sp, x = lax.axis_index("sp"), lax.axis_index("tp")
    z, p = sp // PLANE, lax.rem(sp, PLANE)
    z_up = lax.rem(z + 1, NZ) * PLANE + p
    z_down = lax.rem(z + NZ - 1, NZ) * PLANE + p
    x_up, x_down, x_far = lax.rem(x + 1, NX), lax.rem(x + NX - 1, NX), lax.rem(x + 2, NX)
    up, down = (z_up, x), (z_down, x)
    right, left, far = (sp, x_up), (sp, x_down), (sp, x_far)
    ahead = [(z * PLANE + lax.rem(p + q, PLANE), x) for q in range(PLANE)]
    behind = [(z * PLANE + lax.rem(p + PLANE - q, PLANE), x) for q in range(PLANE)]
    net = Net(sems)
    narrow = [k for k in range(CHUNKS) if k not in WIDE]
    place = {k: (scr_wide, WIDE.index(k), NX) if k in WIDE else (scr_narrow, narrow.index(k), 1) for k in range(CHUNKS)}

    def buf(k, name):
        group, i, _ = place[k]
        return group[name].at[i]

    def cols(k):
        return slice(k * width, (k + 1) * width)

    weight_copies = [
        pltpu.make_async_copy(src.at[0], dst, wsem.at[i])
        for i, (src, dst) in enumerate(((wg_hbm, wg), (wu_hbm, wu), (wd_hbm, wd)))
    ]
    project_copy = pltpu.make_async_copy(wo_hbm, wo, wsem.at[3])
    project_copy.start()
    for copy in weight_copies:
        copy.start()

    meta[0, 0] = meta_ref[...]
    held = kv_ref.shape[0]
    lanes = 2 * HEAD

    def head_mean(squares):
        r = lax.broadcasted_iota(jnp.int32, (lanes, lanes), 0) // HEAD
        c = lax.broadcasted_iota(jnp.int32, (lanes, lanes), 1) // HEAD
        spread_out = jnp.where(r == c, 1.0 / HEAD, 0.0).astype(f32)
        return jnp.dot(squares, spread_out, preferred_element_type=f32, precision=lax.Precision.HIGHEST)

    def normed_rotated(value, gain):
        scaled = value * lax.rsqrt(head_mean(value * value) + norm_eps) * gain
        lane = lax.broadcasted_iota(jnp.int32, value.shape, 1)
        first = lax.rem(lane, HEAD) < HEAD // 2
        turned = jnp.where(
            first, -pltpu.roll(scaled, lanes - HEAD // 2, axis=1), pltpu.roll(scaled, HEAD // 2, axis=1)
        )
        return scaled * angle_ref[:, :lanes] + turned * angle_ref[:, lanes:]

    own = pl.ds(WINDOW, held)
    kv = kv_ref[...].astype(f32)
    on_key = lax.broadcasted_iota(jnp.int32, kv.shape, 1) < HEAD
    kv_span[own, :] = jnp.where(on_key, normed_rotated(kv, gain_ref[1:2, :]), kv).astype(bf16)
    doc_span[:, own] = doc_ref[...]

    barrier = pltpu.get_barrier_semaphore()
    count = NZ * PLANE
    after, before = (lax.rem(sp + 1, count), x), (lax.rem(sp + count - 1, count), x)
    peers = [up, down, right, left, after, before, far] + ahead[1:]
    for peer in peers:
        pl.semaphore_signal(barrier, inc=1, device_id=peer, device_id_type=MESH)
    pl.semaphore_wait(barrier, len(peers))

    low_rows, high_rows = pl.ds(0, WINDOW), pl.ds(held + WINDOW, WINDOW)
    net.send("kv+", kv_span.at[pl.ds(held, WINDOW), :], kv_span.at[low_rows, :], after)
    net.send("kv-", kv_span.at[pl.ds(WINDOW, WINDOW), :], kv_span.at[high_rows, :], before)
    net.send("doc+", doc_ref.at[:, pl.ds(held - WINDOW, WINDOW)], doc_span.at[:, low_rows], after)
    net.send("doc-", doc_ref.at[:, pl.ds(0, WINDOW)], doc_span.at[:, high_rows], before)
    pairs = q_ref.shape[1] // lanes
    for i in range(pairs):
        part = slice(i * lanes, (i + 1) * lanes)
        q_rot[:, part] = normed_rotated(q_ref[:, part].astype(f32), gain_ref[0:1, :]).astype(bf16)
    for name in ("kv+", "kv-", "doc+", "doc-"):
        net.arrived(name)
    both = kv_span[...].astype(f32)
    swapped = pltpu.roll(both, HEAD, axis=1)
    on_key = lax.broadcasted_iota(jnp.int32, both.shape, 1) < HEAD
    key_twice = jnp.where(on_key, both, swapped).astype(bf16)
    value_twice = jnp.where(on_key, swapped, both).astype(bf16)
    span = held + 2 * WINDOW
    query_at = lax.broadcasted_iota(jnp.int32, (held, span), 0)
    key_at = lax.broadcasted_iota(jnp.int32, (held, span), 1) - WINDOW
    place_at = sp * held + key_at
    allowed = (jnp.abs(query_at - key_at) <= WINDOW) & (place_at >= 0) & (place_at < count * held)
    allowed = allowed & (doc_ref[...].T[:, 0:1] == doc_span[0:1, :])
    in_first = lax.broadcasted_iota(jnp.int32, (held, lanes), 1) < HEAD
    for i in range(pairs):
        mixed_pair = []
        for j in range(2):
            q = q_rot[:, i * lanes : (i + 1) * lanes]
            q = jnp.where(in_first if j == 0 else ~in_first, q.astype(f32), 0.0).astype(bf16)
            scores = lax.dot_general(q, key_twice, (((1,), (1,)), ((), ())), preferred_element_type=f32)
            raw = jnp.where(allowed, jnp.exp(scores * HEAD ** (-0.5)), 0.0)
            h = 2 * i + j
            total = jnp.sum(raw, axis=1, keepdims=True) + jnp.exp(sink_ref[0:1, h : h + 1])
            mixed_pair.append(jnp.dot((raw / total).astype(bf16), value_twice, preferred_element_type=f32))
        att[:, i * lanes : (i + 1) * lanes] = jnp.where(in_first, mixed_pair[0], mixed_pair[1]).astype(bf16)
    for d, peer in ((2, far), (1, right), (3, left)):
        other = pl.multiple_of(lax.rem(x + d, NX) * toks, toks)
        net.send(("att", d), att.at[pl.ds(other, toks), :], by_token.at[x], peer)
    by_token[x] = att[pl.ds(pl.multiple_of(x * toks, toks), toks), :]
    project_copy.wait()
    for d in (1, 2, 3):
        net.arrived(("att", d))
    channels = att.shape[1]
    pieces = [by_token[i].astype(f32) for i in range(NX)]
    square = sum(jnp.sum(piece * piece, axis=1, keepdims=True) for piece in pieces)
    inverse = lax.rsqrt(square / (NX * channels) + norm_eps)
    pieces = [
        (piece * inverse * out_gain_ref[0:1, i * channels : (i + 1) * channels]).astype(bf16)
        for i, piece in enumerate(pieces)
    ]
    for k in range(CHUNKS):
        made = resid_ref[:, cols(k)].astype(f32)
        made = made + sum(
            jnp.dot(piece, wo[i * channels : (i + 1) * channels, cols(k)], preferred_element_type=f32)
            for i, piece in enumerate(pieces)
        )
        mid_ref[:, cols(k)] = made.astype(bf16)
    square = jnp.zeros((toks, 1), f32)
    for k in range(CHUNKS):
        value = mid_ref[:, cols(k)].astype(f32)
        square = square + jnp.sum(value * value, axis=1, keepdims=True)
    inverse = lax.rsqrt(square / model + norm_eps)
    for k in range(CHUNKS):
        value = mid_ref[:, cols(k)].astype(f32) * inverse * norm_gain_ref[0:1, cols(k)]
        buf(k, "spread")[0, 0] = value.astype(bf16)

    meta_width = NX if WIDE else 1

    def up_hops(k):
        return 4 if k % 2 == 0 else 3

    def up_slot(h):
        return h

    def down_slot(h):
        return 4 if h == 4 else (0 if h == 0 else 4 + h)

    def wide_first(k):
        spread = buf(k, "spread")
        src = spread.at[0, 0]
        net.send((k, "w", 1), src, spread.at[0, 1], right)
        net.send((k, "w", 2), src, spread.at[0, 2], left)
        net.send((k, "w", 3), src, spread.at[0, 3], far)

    def meta_first():
        if WIDE:
            net.send(("mw", 1), meta_ref, meta.at[0, 1], right)
            net.send(("mw", 2), meta_ref, meta.at[0, 2], left)
            net.send(("mw", 3), meta_ref, meta.at[0, 3], far)

    def ring_hop(name, h, last_up, last_down, data):
        if h <= last_up:
            if h > 1:
                net.arrived((name, "u", h - 1))
            net.send((name, "u", h), data.at[up_slot(h - 1)], data.at[up_slot(h)], up)
        if h <= last_down:
            if h > 1:
                net.arrived((name, "d", h - 1))
            net.send((name, "d", h), data.at[down_slot(h - 1)], data.at[down_slot(h)], down)

    def meta_hop(h):
        ring_hop("m", h, 4, 3, meta.at[:, 0])

    def meta_wide_hop(h):
        if h == 1:
            for i in (1, 2, 3):
                net.arrived(("mw", i))
        ring_hop("mz", h, 4, 3, meta.at[:, pl.ds(1, NX - 1)])

    def token_hop(k, h):
        if h == 1 and k in WIDE:
            for i in (1, 2, 3):
                net.arrived((k, "w", i))
        ring_hop(k, h, up_hops(k), 7 - up_hops(k), buf(k, "spread"))

    def tables(others):
        indices = range(1, NX) if others else (0,)
        net.arrived(("mz" if others else "m", "u", 4))
        net.arrived(("mz" if others else "m", "d", 3))
        shape = (2 * toks, 2 * toks)
        row = lax.broadcasted_iota(jnp.int32, shape, 0)
        lane = lax.broadcasted_iota(jnp.int32, shape, 1)
        expert = z * PLANE + lax.rem(p + row // 16, PLANE)
        target = (expert * CAP + lax.rem(row, CAP)).astype(f32)
        second = lane >= toks
        valid = (lax.rem(row // CAP, 2) == 1) == second
        low = lax.broadcasted_iota(jnp.int32, (16, 2 * toks), 1) < toks
        for xi in indices:
            for i in range(NZ // 2):
                both = jnp.where(low, meta[2 * i, xi], meta[2 * i + 1, xi])
                chosen = jnp.zeros(shape, f32)
                weighted = jnp.zeros(shape, f32)
                for r in range(4):
                    hit = (both[r : r + 1, :] == target) & valid
                    chosen = jnp.where(hit, 1.0, chosen)
                    weighted = jnp.where(hit, both[8 + r : 9 + r, :], weighted)
                pick[xi, i] = chosen.astype(bf16)
                mixed = weighted.T
                high = mixed.astype(bf16)
                mix_hi[xi, i] = high
                mix_lo[xi, i] = (mixed - high.astype(f32)).astype(bf16)

    def select(k):
        net.arrived((k, "u", up_hops(k)))
        net.arrived((k, "d", 7 - up_hops(k)))
        spread, chosen = buf(k, "spread"), buf(k, "chosen")
        for xi in range(place[k][2]):
            for i in range(NZ // 2):
                pair = jnp.concatenate([spread[2 * i, xi], spread[2 * i + 1, xi]], axis=0)
                got = jnp.dot(pick[xi, i], pair, preferred_element_type=f32).astype(bf16)
                rows[k, xi, 16 * i : 16 * i + 16, :] = got[0:16]
                for q in range(1, PLANE):
                    chosen[q - 1, xi, 16 * i : 16 * i + 16, :] = got[16 * q : 16 * q + 16]
        for q in (4, 5, 2, 3, 6, 7, 1):
            net.send(
                (k, "y", q), chosen.at[q - 1],
                rows.at[k, pl.ds(0, place[k][2]), pl.ds(q * toks, toks), :], ahead[q],
            )

    def gather_rows(k):
        first, second = pl.ds(0, half), pl.ds(half, half)
        for q in range(1, PLANE // 2):
            net.arrived((k, "y", q))
        net.send((k, "rA"), rows.at[k, 0, first, :], rows.at[k, 1, first, :], right)
        for q in range(PLANE // 2, PLANE):
            net.arrived((k, "y", q))
        net.send((k, "lB"), rows.at[k, 0, second, :], rows.at[k, 2, second, :], left)
        net.send((k, "rB"), rows.at[k, 0, second, :], rows.at[k, 1, second, :], right)
        net.send((k, "lA"), rows.at[k, 0, first, :], rows.at[k, 2, first, :], left)

    def forward_rows(k):
        first, second = pl.ds(0, half), pl.ds(half, half)
        net.arrived((k, "rA"))
        net.send((k, "fA"), rows.at[k, 1, first, :], rows.at[k, 3, first, :], right)
        net.arrived((k, "lB"))
        net.send((k, "fB"), rows.at[k, 2, second, :], rows.at[k, 3, second, :], left)

    def expert_in(k, first, last):
        if k in WIDE:
            for q in range(1, PLANE):
                net.arrived((k, "y", q))
        else:
            for name in ("rB", "lA", "fA", "fB"):
                net.arrived((k, name))
        if first:
            weight_copies[0].wait()
            weight_copies[1].wait()

        def tile(i, _):
            xi, part = i // 2, lax.rem(i, 2)
            a = rows[k, xi, pl.ds(pl.multiple_of(part * half, half), half), :]
            at = pl.ds(pl.multiple_of(i * half, half), half)
            g = jnp.dot(a, wg[cols(k), :], preferred_element_type=f32)
            u = jnp.dot(a, wu[cols(k), :], preferred_element_type=f32)
            if not first:
                g = g + gate_acc[at, :]
                u = u + up_acc[at, :]
            if last:
                c = jnp.minimum(g, swiglu_limit)
                u = jnp.clip(u, -swiglu_limit, swiglu_limit)
                hidden[at, :] = ((u + 1.0) * c * jax.nn.sigmoid(swiglu_alpha * c)).astype(bf16)
            else:
                gate_acc[at, :] = g
                up_acc[at, :] = u
            return 0

        lax.fori_loop(0, 2 * NX, tile, 0)

    def expert_out(k, first):
        if first:
            weight_copies[2].wait()
        for q in range(1, PLANE):
            net.sent((k, "y", q))
        if k not in WIDE:
            for name in ("rA", "lB", "rB", "lA", "fA", "fB"):
                net.sent((k, name))

        def tile(i, _):
            xi, part = i // 2, lax.rem(i, 2)
            at = pl.ds(pl.multiple_of(i * half, half), half)
            made = jnp.dot(hidden[at, :], wd[:, cols(k)], preferred_element_type=f32)
            rows[k, xi, pl.ds(pl.multiple_of(part * half, half), half), :] = made.astype(bf16)
            return 0

        lax.fori_loop(0, 2 * NX, tile, 0)
        a, b = pl.ds(0, half), pl.ds(half, half)
        if k in WIDE:
            back = buf(k, "back")
            for q in (4, 5, 2, 3, 6, 7, 1):
                net.send((k, "b", q), rows.at[k, pl.ds(0, NX), pl.ds(q * toks, toks), :], back.at[q - 1], behind[q])
        else:
            net.send((k, "oA"), rows.at[k, 3, a, :], buf(k, "hop_r"), right)
            net.send((k, "oB"), rows.at[k, 3, b, :], buf(k, "hop_l"), left)
            net.send((k, "dB"), rows.at[k, 2, b, :], buf(k, "sum_r").at[b, :], right)
            net.send((k, "dA"), rows.at[k, 1, a, :], buf(k, "sum_l").at[a, :], left)

    def reduce_hop(k):
        a, b = pl.ds(0, half), pl.ds(half, half)
        net.arrived((k, "oA"))
        rows[k, 2, a, :] = (rows[k, 2, a, :].astype(f32) + buf(k, "hop_r")[...].astype(f32)).astype(bf16)
        net.send((k, "sA"), rows.at[k, 2, a, :], buf(k, "sum_r").at[a, :], right)
        net.arrived((k, "oB"))
        rows[k, 1, b, :] = (rows[k, 1, b, :].astype(f32) + buf(k, "hop_l")[...].astype(f32)).astype(bf16)
        net.send((k, "sB"), rows.at[k, 1, b, :], buf(k, "sum_l").at[b, :], left)

    def reduce_rows(k):
        for name in ("dB", "dA", "sA", "sB"):
            net.arrived((k, name))
        back, total = buf(k, "back"), buf(k, "total")
        total[...] = (
            rows[k, 0].astype(f32) + buf(k, "sum_r")[...].astype(f32) + buf(k, "sum_l")[...].astype(f32)
        ).astype(bf16)
        for q in (4, 5, 2, 3, 6, 7, 1):
            net.send((k, "b", q), total.at[pl.ds(q * toks, toks), :], back.at[q - 1, 0], behind[q])

    def combine(k):
        for q in range(1, PLANE):
            net.arrived((k, "b", q))
        back, mixed = buf(k, "back"), buf(k, "mixed")
        for xi in range(place[k][2]):
            for i in range(NZ // 2):
                part = slice(16 * i, 16 * i + 16)
                own = rows[k, xi, part, :] if k in WIDE else buf(k, "total")[part, :]
                outs = jnp.concatenate([own] + [back[q - 1, xi, part, :] for q in range(1, PLANE)], axis=0)
                got = jnp.dot(mix_hi[xi, i], outs, preferred_element_type=f32)
                got = got + jnp.dot(mix_lo[xi, i], outs, preferred_element_type=f32)
                mixed[2 * i, xi] = got[:toks]
                mixed[2 * i + 1, xi] = got[toks:]

    def return_hop(k, h):
        mixed, leaving = buf(k, "mixed"), buf(k, "leaving")
        for way, hops, slot, landing, to in (
            ("D", up_hops(k), up_slot, buf(k, "from_up"), down),
            ("U", 7 - up_hops(k), down_slot, buf(k, "from_down"), up),
        ):
            j = hops - h + 1
            if j < 1:
                continue
            value = mixed[slot(j)]
            if h > 1:
                net.arrived((k, way, h - 1))
                value = value + landing[j].astype(f32)
            leaving[slot(j)] = value.astype(bf16)
            net.send((k, way, h), leaving.at[slot(j)], landing.at[j - 1], to)

    def finish(k):
        mixed = buf(k, "mixed")
        net.arrived((k, "D", up_hops(k)))
        net.arrived((k, "U", 7 - up_hops(k)))
        value = mixed[0] + buf(k, "from_up")[0].astype(f32) + buf(k, "from_down")[0].astype(f32)
        if k in WIDE:
            mixed[0] = value
            leaving = buf(k, "leaving")
            leaving[0] = value.astype(bf16)
            last = buf(k, "last")
            net.send((k, "X", 2), leaving.at[0, 2], last.at[2], right)
            net.send((k, "X", 1), leaving.at[0, 1], last.at[1], left)
            net.send((k, "X", 3), leaving.at[0, 3], last.at[3], far)
        else:
            out_ref[:, cols(k)] = (mid_ref[:, cols(k)].astype(f32) + value[0]).astype(bf16)

    def finish_wide(k):
        mixed, last = buf(k, "mixed"), buf(k, "last")
        value = mixed[0, 0]
        for i in (1, 2, 3):
            net.arrived((k, "X", i))
            value = value + last[i].astype(f32)
        out_ref[:, cols(k)] = (mid_ref[:, cols(k)].astype(f32) + value).astype(bf16)

    steps = (
        meta_first, meta_hop, meta_wide_hop, tables, wide_first, token_hop, select, gather_rows, forward_rows,
        expert_in, expert_out, reduce_hop, reduce_rows, combine, return_hop, finish, finish_wide,
    )
    done = {step: 0 for step in steps}
    for number, *args in ORDER:
        step = steps[number]
        if step is expert_in:
            args = args + [done[step] == 0, done[step] == CHUNKS - 1]
        if step is expert_out:
            args = args + [done[step] == 0]
        done[step] += 1
        step(*args)
    for name in net.copies:
        net.sent(name)
    assert net.used == sems.shape[0], net.used


def layer(queries, key_value, doc_rows, angles, gains, sink, out_gain, norm_gain, resid, meta, w_out, w_gate, w_up, w_down):
    bf16, f32 = jnp.bfloat16, jnp.float32
    toks, model = resid.shape
    held, channels = queries.shape
    width = model // CHUNKS
    units = w_gate.shape[2]
    block = PLANE * toks
    wides = len(WIDE)
    meta_width = NX if WIDE else 1

    def group(count, nx):
        if count == 0:
            return {"none": pltpu.VMEM((16, 128), bf16)}
        shapes = {
            "spread": pltpu.VMEM((count, NZ, nx, toks, width), bf16),
            "chosen": pltpu.VMEM((count, PLANE - 1, nx, toks, width), bf16),
            "back": pltpu.VMEM((count, PLANE - 1, nx, toks, width), bf16),
            "mixed": pltpu.VMEM((count, NZ, nx, toks, width), f32),
            "leaving": pltpu.VMEM((count, NZ, nx, toks, width), bf16),
            "from_up": pltpu.VMEM((count, 4, nx, toks, width), bf16),
            "from_down": pltpu.VMEM((count, 4, nx, toks, width), bf16),
        }
        if nx == 1:
            shapes["hop_r"] = pltpu.VMEM((count, block // 2, width), bf16)
            shapes["hop_l"] = pltpu.VMEM((count, block // 2, width), bf16)
            shapes["sum_r"] = pltpu.VMEM((count, block, width), bf16)
            shapes["sum_l"] = pltpu.VMEM((count, block, width), bf16)
            shapes["total"] = pltpu.VMEM((count, block, width), bf16)
        else:
            shapes["last"] = pltpu.VMEM((count, nx, toks, width), bf16)
        return shapes

    per_narrow = 7 + 7 + 6 + 6 + 7 + 7
    per_wide = 3 + 7 + 7 + 7 + 7 + 3
    copies = 7 + 7 + (10 if WIDE else 0) + (CHUNKS - wides) * per_narrow + wides * per_wide
    any_spec = pl.BlockSpec(memory_space=pl.ANY)
    vmem_spec = pl.BlockSpec(memory_space=pltpu.VMEM)
    narrow_shapes, wide_shapes = group(CHUNKS - wides, 1), group(wides, NX)
    names_n, names_w = list(narrow_shapes), list(wide_shapes)

    def body(*refs):
        fixed, rest = refs[:33], refs[33:]
        scr_n = dict(zip(names_n, rest[: len(names_n)]))
        rest = rest[len(names_n) :]
        scr_w = dict(zip(names_w, rest[: len(names_w)]))
        sems, wsem = rest[len(names_w) :]
        moe_kernel(*fixed, scr_n, scr_w, sems, wsem)

    tables = [pltpu.VMEM((meta_width, NZ // 2, 2 * toks, 2 * toks), bf16) for _ in range(3)]
    return pl.pallas_call(
        body,
        out_shape=jax.ShapeDtypeStruct((toks, model), bf16),
        in_specs=[vmem_spec] * 10 + [any_spec] * 4,
        out_specs=vmem_spec,
        scratch_shapes=[
            pltpu.VMEM(w_out.shape, bf16),
            pltpu.VMEM((held, channels), bf16),
            pltpu.VMEM((held + 2 * WINDOW, 2 * HEAD), bf16),
            pltpu.VMEM((8, held + 2 * WINDOW), f32),
            pltpu.VMEM((held, channels), bf16),
            pltpu.VMEM((NX, toks, channels), bf16),
            pltpu.VMEM((toks, model), bf16),
            pltpu.VMEM((model, units), bf16),
            pltpu.VMEM((model, units), bf16),
            pltpu.VMEM((units, model), bf16),
            pltpu.VMEM((CHUNKS, NX, block, width), bf16),
            pltpu.VMEM((NX * block, units), f32),
            pltpu.VMEM((NX * block, units), f32),
            pltpu.VMEM((NX * block, units), bf16),
            pltpu.VMEM((NZ, meta_width, 16, 2 * toks), f32),
            *tables,
            *narrow_shapes.values(),
            *wide_shapes.values(),
            pltpu.SemaphoreType.DMA((2 * copies,)),
            pltpu.SemaphoreType.DMA((4,)),
        ],
        compiler_params=pltpu.CompilerParams(
            collective_id=0, has_side_effects=True, vmem_limit_bytes=VMEM_LIMIT
        ),
        name="layer",
    )(queries, key_value, doc_rows, angles, gains, sink, out_gain, norm_gain, resid, meta, w_out, w_gate, w_up, w_down)


def route_table(own_routes, weights):
    routes = own_routes.T
    top, toks = routes.shape
    ids = jnp.arange(toks, dtype=jnp.int32)
    same = routes[:, :, None, None] == routes[None, None, :, :]
    earlier = ids[None, None, None, :] < ids[None, :, None, None]
    rank = jnp.sum((same & earlier).astype(jnp.int32), axis=(2, 3))
    slots = (routes * CAP + rank).astype(jnp.float32)
    pad = jnp.full((8 - top, toks), -1.0, jnp.float32)
    table = jnp.concatenate([slots, pad, weights.T, pad], axis=0)
    return jnp.concatenate([table, table], axis=1)


def per_device(
    resid,
    queries,
    keys,
    values,
    docs,
    q_gain,
    key_norm_gain,
    sink,
    out_gain,
    w_out,
    norm_gain,
    routes,
    route_weights,
    w_gate,
    w_up,
    w_down,
):
    tp_size = lax.axis_size("tp")
    sp_index = lax.axis_index("sp")
    tp_index = lax.axis_index("tp")
    f32 = jnp.float32
    held = queries.shape[0]
    positions = (sp_index * held + jnp.arange(held, dtype=jnp.int32)).astype(f32)
    half = HEAD // 2
    freqs = rope_base ** (-jnp.arange(half, dtype=f32) / half)
    turns = positions[:, None] * jnp.tile(freqs, 2 * HEAD // half)[None, :]
    angles = jnp.concatenate([jnp.cos(turns), jnp.sin(turns)], axis=1)
    gains = jnp.stack([jnp.tile(q_gain, 2), jnp.tile(key_norm_gain, 2)])
    quarter = held // lax.axis_size("tp")
    own_routes = lax.dynamic_slice_in_dim(routes, tp_index * quarter, quarter, 0)
    return layer(
        queries,
        jnp.concatenate([keys, values], axis=1),
        jnp.broadcast_to(docs.astype(f32)[None, :], (8, held)),
        angles,
        gains,
        sink[None, :],
        out_gain[None, :],
        norm_gain[None, :],
        resid,
        route_table(own_routes, route_weights),
        w_out,
        w_gate,
        w_up,
        w_down,
    )


def solution(mesh):
    return jax.shard_map(
        per_device,
        mesh=mesh,
        in_specs=(
            P(("sp", "tp"), None),
            P("sp", "tp"),
            P("sp", "tp"),
            P("sp", "tp"),
            P("sp"),
            P(),
            P(),
            P("tp"),
            P(),
            P(),
            P(),
            P("sp", None),
            P(("sp", "tp"), None),
            P("sp", None, "tp"),
            P("sp", None, "tp"),
            P("sp", "tp", None),
        ),
        out_specs=P(("sp", "tp"), None),
        check_vma=False,
    )
```

```python
import jax
import jax.numpy as jnp
from jax import lax
from jax.experimental import pallas as pl
from jax.experimental.pallas import tpu as pltpu
from jax.sharding import PartitionSpec as P

WINDOW = 128
MESH = pl.DeviceIdType.MESH

NZ = 8
PLANE = 8
NX = 4
CAP = 8
HEAD = 64
CHUNKS = 8
WIDE = (6, 7)
VMEM_LIMIT = 67_043_328
ORDER = (
    (0,), (1, 1), (5, 1, 1), (5, 0, 1), (4, 7), (1, 2), (4, 6), (5, 1, 2), (5, 3, 1), (1, 3), (5, 1, 3), (5, 0, 2),
    (1, 4), (5, 1, 4), (5, 4, 1), (2, 1), (5, 0, 3), (3, 0), (5, 2, 1), (6, 1), (5, 4, 2), (5, 0, 4), (5, 5, 1),
    (5, 3, 2), (5, 2, 2), (5, 4, 3), (7, 1), (5, 7, 1), (6, 0), (5, 4, 4), (8, 1), (5, 3, 3), (2, 2), (5, 3, 4),
    (5, 5, 2), (7, 0), (5, 7, 2), (5, 2, 3), (6, 4), (2, 3), (6, 3), (8, 0), (5, 5, 3), (5, 2, 4), (7, 4),
    (5, 7, 3), (5, 5, 4), (6, 2), (2, 4), (7, 3), (5, 6, 1), (5, 7, 4), (6, 5), (5, 6, 2), (8, 4), (7, 2), (3, 1),
    (8, 3), (6, 7), (5, 6, 3), (9, 0), (8, 2), (5, 6, 4), (9, 4), (9, 1), (6, 6), (7, 5), (9, 2), (8, 5), (9, 7),
    (9, 3), (9, 5), (9, 6), (10, 6), (10, 7), (10, 0), (10, 1), (11, 1), (11, 0), (10, 2), (10, 3), (13, 6),
    (14, 6, 1), (12, 0), (14, 6, 2), (13, 7), (14, 7, 1), (12, 1), (13, 0), (14, 0, 1), (14, 7, 2), (11, 3),
    (11, 2), (13, 1), (10, 4), (14, 6, 3), (12, 3), (14, 1, 1), (14, 7, 3), (12, 2), (11, 4), (14, 1, 2),
    (14, 0, 2), (14, 6, 4), (10, 5), (14, 7, 4), (13, 2), (14, 2, 1), (12, 4), (13, 3), (14, 3, 1), (14, 1, 3),
    (11, 5), (14, 0, 3), (14, 2, 2), (15, 6), (13, 4), (14, 4, 1), (14, 1, 4), (12, 5), (14, 3, 2), (14, 0, 4),
    (15, 7), (14, 4, 2), (14, 2, 3), (13, 5), (14, 5, 1), (16, 6), (14, 4, 3), (14, 5, 2), (14, 3, 3), (14, 5, 3),
    (14, 4, 4), (14, 2, 4), (15, 1), (15, 0), (14, 3, 4), (14, 5, 4), (15, 4), (15, 3), (16, 7), (15, 2), (15, 5),
)


rope_base = 10000.0
norm_eps = 1e-06
swiglu_limit = 7.0
swiglu_alpha = 1.702


class Net:
    def __init__(self, sems):
        self.sems = sems
        self.used = 0
        self.copies = {}
        self.groups = {}

    def semaphore(self):
        self.used += 1
        return self.sems.at[self.used - 1]

    def group(self, kind, key, whole, device):
        if (kind, key) not in self.groups:
            sem = self.semaphore()
            copy = pltpu.make_async_remote_copy(
                src_ref=whole, dst_ref=whole, send_sem=sem, recv_sem=sem, device_id=device, device_id_type=MESH
            )
            self.groups[kind, key] = [sem, copy, False]
        return self.groups[kind, key][0]

    def send(self, name, src, dst, device, out=None, into=None):
        copy = pltpu.make_async_remote_copy(
            src_ref=src,
            dst_ref=dst,
            send_sem=self.group("out", *out, device) if out else self.semaphore(),
            recv_sem=self.group("into", *into, device) if into else self.semaphore(),
            device_id=device,
            device_id_type=MESH,
        )
        copy.start()
        self.copies[name] = (copy, out is None)

    def arrived(self, name):
        self.copies[name][0].wait_recv()

    def all_arrived(self, key):
        self.groups["into", key][1].wait_recv()

    def all_sent(self, key):
        group = self.groups["out", key]
        if not group[2]:
            group[1].wait_send()
            group[2] = True

    def finish(self):
        for kind, key in self.groups:
            if kind == "out":
                self.all_sent(key)
        for copy, alone in self.copies.values():
            if alone:
                copy.wait_send()


def moe_kernel(
    q_ref, key_ref, value_ref, doc_ref, cos_ref, sin_ref, q_gain_ref, k_gain_ref, sink_ref, out_gain_ref,
    norm_gain_ref, resid_ref, slot_ref, weight_ref,
    wo_hbm, wg_hbm, wu_hbm, wd_hbm, out_ref,
    wo, q_rot, kv_span, doc_span, att, by_token, mid_ref,
    wg, wu, wd, rows, gate_acc, up_acc, hidden, meta, pick, mix_hi, mix_lo,
    scr_narrow, scr_wide, sems, wsem,
):
    bf16, f32 = jnp.bfloat16, jnp.float32
    toks, model = resid_ref.shape
    width = model // CHUNKS
    block = PLANE * toks
    half = block // 2
    sp, x = lax.axis_index("sp"), lax.axis_index("tp")
    z, p = sp // PLANE, lax.rem(sp, PLANE)
    z_up = lax.rem(z + 1, NZ) * PLANE + p
    z_down = lax.rem(z + NZ - 1, NZ) * PLANE + p
    x_up, x_down, x_far = lax.rem(x + 1, NX), lax.rem(x + NX - 1, NX), lax.rem(x + 2, NX)
    up, down = (z_up, x), (z_down, x)
    right, left, far = (sp, x_up), (sp, x_down), (sp, x_far)
    ahead = [(z * PLANE + lax.rem(p + q, PLANE), x) for q in range(PLANE)]
    behind = [(z * PLANE + lax.rem(p + PLANE - q, PLANE), x) for q in range(PLANE)]
    net = Net(sems)
    narrow = [k for k in range(CHUNKS) if k not in WIDE]
    place = {k: (scr_wide, WIDE.index(k), NX) if k in WIDE else (scr_narrow, narrow.index(k), 1) for k in range(CHUNKS)}

    def buf(k, name):
        group, i, _ = place[k]
        return group[name].at[i]

    def cols(k):
        return slice(k * width, (k + 1) * width)

    weight_copies = [
        pltpu.make_async_copy(src.at[0], dst, wsem.at[i])
        for i, (src, dst) in enumerate(((wg_hbm, wg), (wu_hbm, wu), (wd_hbm, wd)))
    ]
    project_copy = pltpu.make_async_copy(wo_hbm, wo, wsem.at[3])
    project_copy.start()
    for copy in weight_copies:
        copy.start()

    held = q_ref.shape[0]
    table = jnp.concatenate([slot_ref[...], weight_ref[...]], axis=0)
    table = jnp.concatenate([table, table], axis=1)
    meta[0, 0] = jnp.concatenate([table, table], axis=0)
    lanes = 2 * HEAD

    def head_mean(squares):
        r = lax.broadcasted_iota(jnp.int32, (lanes, lanes), 0) // HEAD
        c = lax.broadcasted_iota(jnp.int32, (lanes, lanes), 1) // HEAD
        spread_out = jnp.where(r == c, 1.0 / HEAD, 0.0).astype(f32)
        return jnp.dot(squares, spread_out, preferred_element_type=f32, precision=lax.Precision.HIGHEST)

    def normed_rotated(value, gain):
        scaled = value * lax.rsqrt(head_mean(value * value) + norm_eps) * gain
        lane = lax.broadcasted_iota(jnp.int32, value.shape, 1)
        first = lax.rem(lane, HEAD) < HEAD // 2
        turned = jnp.where(
            first, -pltpu.roll(scaled, lanes - HEAD // 2, axis=1), pltpu.roll(scaled, HEAD // 2, axis=1)
        )
        return scaled * cos_ref[...] + turned * sin_ref[...]

    own = pl.ds(WINDOW, held)
    kv = jnp.concatenate([key_ref[...], value_ref[...]], axis=0).astype(f32).T
    q_gain = jnp.concatenate([q_gain_ref[...], q_gain_ref[...]], axis=1)
    k_gain = jnp.concatenate([k_gain_ref[...], k_gain_ref[...]], axis=1)
    on_key = lax.broadcasted_iota(jnp.int32, kv.shape, 1) < HEAD
    kv_span[own, :] = jnp.where(on_key, normed_rotated(kv, k_gain), kv).astype(bf16)
    doc_span[:, own] = jnp.broadcast_to(doc_ref[...].astype(f32), (8, held))

    barrier = pltpu.get_barrier_semaphore()
    count = NZ * PLANE
    after, before = (lax.rem(sp + 1, count), x), (lax.rem(sp + count - 1, count), x)
    peers = [up, down, right, left, after, before, far] + ahead[1:]
    for peer in peers:
        pl.semaphore_signal(barrier, inc=1, device_id=peer, device_id_type=MESH)
    pl.semaphore_wait(barrier, len(peers))

    low_rows, high_rows = pl.ds(0, WINDOW), pl.ds(held + WINDOW, WINDOW)
    net.send("kv+", kv_span.at[pl.ds(held, WINDOW), :], kv_span.at[low_rows, :], after)
    net.send("kv-", kv_span.at[pl.ds(WINDOW, WINDOW), :], kv_span.at[high_rows, :], before)
    net.send("doc+", doc_span.at[:, pl.ds(held, WINDOW)], doc_span.at[:, low_rows], after)
    net.send("doc-", doc_span.at[:, pl.ds(WINDOW, WINDOW)], doc_span.at[:, high_rows], before)
    pairs = q_ref.shape[1] // lanes
    for i in range(pairs):
        part = slice(i * lanes, (i + 1) * lanes)
        q_rot[:, part] = normed_rotated(q_ref[:, part].astype(f32), q_gain).astype(bf16)
    for name in ("kv+", "kv-", "doc+", "doc-"):
        net.arrived(name)
    both = kv_span[...].astype(f32)
    swapped = pltpu.roll(both, HEAD, axis=1)
    on_key = lax.broadcasted_iota(jnp.int32, both.shape, 1) < HEAD
    key_twice = jnp.where(on_key, both, swapped).astype(bf16)
    value_twice = jnp.where(on_key, swapped, both).astype(bf16)
    span = held + 2 * WINDOW
    query_at = lax.broadcasted_iota(jnp.int32, (held, span), 0)
    key_at = lax.broadcasted_iota(jnp.int32, (held, span), 1) - WINDOW
    place_at = sp * held + key_at
    allowed = (jnp.abs(query_at - key_at) <= WINDOW) & (place_at >= 0) & (place_at < count * held)
    allowed = allowed & (doc_span[:, own].T[:, 0:1] == doc_span[0:1, :])
    in_first = lax.broadcasted_iota(jnp.int32, (held, lanes), 1) < HEAD
    for i in range(pairs):
        mixed_pair = []
        for j in range(2):
            q = q_rot[:, i * lanes : (i + 1) * lanes]
            q = jnp.where(in_first if j == 0 else ~in_first, q.astype(f32), 0.0).astype(bf16)
            scores = lax.dot_general(q, key_twice, (((1,), (1,)), ((), ())), preferred_element_type=f32)
            raw = jnp.where(allowed, jnp.exp(scores * HEAD ** (-0.5)), 0.0)
            h = 2 * i + j
            total = jnp.sum(raw, axis=1, keepdims=True) + jnp.exp(sink_ref[0:1, h : h + 1])
            mixed_pair.append(jnp.dot((raw / total).astype(bf16), value_twice, preferred_element_type=f32))
        att[:, i * lanes : (i + 1) * lanes] = jnp.where(in_first, mixed_pair[0], mixed_pair[1]).astype(bf16)
    for d, peer in ((2, far), (1, right), (3, left)):
        other = pl.multiple_of(lax.rem(x + d, NX) * toks, toks)
        net.send(("att", d), att.at[pl.ds(other, toks), :], by_token.at[x], peer)
    by_token[x] = att[pl.ds(pl.multiple_of(x * toks, toks), toks), :]
    project_copy.wait()
    for d in (1, 2, 3):
        net.arrived(("att", d))
    channels = att.shape[1]
    pieces = [by_token[i].astype(f32) for i in range(NX)]
    square = sum(jnp.sum(piece * piece, axis=1, keepdims=True) for piece in pieces)
    inverse = lax.rsqrt(square / (NX * channels) + norm_eps)
    pieces = [
        (piece * inverse * out_gain_ref[0:1, i * channels : (i + 1) * channels]).astype(bf16)
        for i, piece in enumerate(pieces)
    ]
    for k in range(CHUNKS):
        made = resid_ref[:, cols(k)].astype(f32)
        made = made + sum(
            jnp.dot(piece, wo[i * channels : (i + 1) * channels, cols(k)], preferred_element_type=f32)
            for i, piece in enumerate(pieces)
        )
        mid_ref[:, cols(k)] = made.astype(bf16)
    square = jnp.zeros((toks, 1), f32)
    for k in range(CHUNKS):
        value = mid_ref[:, cols(k)].astype(f32)
        square = square + jnp.sum(value * value, axis=1, keepdims=True)
    inverse = lax.rsqrt(square / model + norm_eps)
    for k in range(CHUNKS):
        value = mid_ref[:, cols(k)].astype(f32) * inverse * norm_gain_ref[0:1, cols(k)]
        buf(k, "spread")[0, 0] = value.astype(bf16)

    meta_width = NX if WIDE else 1

    def up_hops(k):
        return 4 if k % 2 == 0 else 3

    def up_slot(h):
        return h

    def down_slot(h):
        return 4 if h == 4 else (0 if h == 0 else 4 + h)

    def wide_first(k):
        spread = buf(k, "spread")
        src = spread.at[0, 0]
        out = ((k, "w"), spread.at[0, pl.ds(1, 3)])
        net.send((k, "w", 1), src, spread.at[0, 1], right, out)
        net.send((k, "w", 2), src, spread.at[0, 2], left, out)
        net.send((k, "w", 3), src, spread.at[0, 3], far, out)

    def meta_first():
        if WIDE:
            net.send(("mw", 1), meta.at[0, 0], meta.at[0, 1], right, ("mw", meta.at[0, pl.ds(1, 3)]))
            net.send(("mw", 2), meta.at[0, 0], meta.at[0, 2], left, ("mw", meta.at[0, pl.ds(1, 3)]))
            net.send(("mw", 3), meta.at[0, 0], meta.at[0, 3], far, ("mw", meta.at[0, pl.ds(1, 3)]))

    def ring_hop(name, h, last_up, last_down, data):
        out = ((name, "z"), data.at[pl.ds(1, NZ - 1)])
        if h <= last_up:
            if h > 1:
                net.arrived((name, "u", h - 1))
            net.send((name, "u", h), data.at[up_slot(h - 1)], data.at[up_slot(h)], up, out)
        if h <= last_down:
            if h > 1:
                net.arrived((name, "d", h - 1))
            net.send((name, "d", h), data.at[down_slot(h - 1)], data.at[down_slot(h)], down, out)

    def meta_hop(h):
        ring_hop("m", h, 4, 3, meta.at[:, 0])

    def meta_wide_hop(h):
        if h == 1:
            for i in (1, 2, 3):
                net.arrived(("mw", i))
        ring_hop("mz", h, 4, 3, meta.at[:, pl.ds(1, NX - 1)])

    def token_hop(k, h):
        if h == 1 and k in WIDE:
            for i in (1, 2, 3):
                net.arrived((k, "w", i))
        ring_hop(k, h, up_hops(k), 7 - up_hops(k), buf(k, "spread"))

    def tables(others):
        indices = range(1, NX) if others else (0,)
        net.arrived(("mz" if others else "m", "u", 4))
        net.arrived(("mz" if others else "m", "d", 3))
        shape = (2 * toks, 2 * toks)
        row = lax.broadcasted_iota(jnp.int32, shape, 0)
        lane = lax.broadcasted_iota(jnp.int32, shape, 1)
        expert = z * PLANE + lax.rem(p + row // 16, PLANE)
        target = (expert * CAP + lax.rem(row, CAP)).astype(f32)
        second = lane >= toks
        valid = (lax.rem(row // CAP, 2) == 1) == second
        low = lax.broadcasted_iota(jnp.int32, (16, 2 * toks), 1) < toks
        for xi in indices:
            for i in range(NZ // 2):
                both = jnp.where(low, meta[2 * i, xi], meta[2 * i + 1, xi])
                chosen = jnp.zeros(shape, f32)
                weighted = jnp.zeros(shape, f32)
                for r in range(4):
                    hit = (both[r : r + 1, :] == target) & valid
                    chosen = jnp.where(hit, 1.0, chosen)
                    weighted = jnp.where(hit, both[4 + r : 5 + r, :], weighted)
                pick[xi, i] = chosen.astype(bf16)
                mixed = weighted.T
                high = mixed.astype(bf16)
                mix_hi[xi, i] = high
                mix_lo[xi, i] = (mixed - high.astype(f32)).astype(bf16)

    def select(k):
        net.arrived((k, "u", up_hops(k)))
        net.arrived((k, "d", 7 - up_hops(k)))
        spread, chosen = buf(k, "spread"), buf(k, "chosen")
        for xi in range(place[k][2]):
            for i in range(NZ // 2):
                pair = jnp.concatenate([spread[2 * i, xi], spread[2 * i + 1, xi]], axis=0)
                got = jnp.dot(pick[xi, i], pair, preferred_element_type=f32).astype(bf16)
                rows[k, xi, 16 * i : 16 * i + 16, :] = got[0:16]
                for q in range(1, PLANE):
                    chosen[q - 1, xi, 16 * i : 16 * i + 16, :] = got[16 * q : 16 * q + 16]
        for q in (4, 5, 2, 3, 6, 7, 1):
            net.send(
                (k, "y", q), chosen.at[q - 1],
                rows.at[k, pl.ds(0, place[k][2]), pl.ds(q * toks, toks), :], ahead[q],
                ((k, "y"), chosen), ((k, "y"), chosen),
            )

    def gather_rows(k):
        first, second = pl.ds(0, half), pl.ds(half, half)
        net.all_arrived((k, "y"))
        out = ((k, "x"), rows.at[k, pl.ds(0, 3)])
        net.send((k, "rA"), rows.at[k, 0, first, :], rows.at[k, 1, first, :], right, out)
        net.send((k, "lB"), rows.at[k, 0, second, :], rows.at[k, 2, second, :], left, out)
        net.send((k, "rB"), rows.at[k, 0, second, :], rows.at[k, 1, second, :], right, out)
        net.send((k, "lA"), rows.at[k, 0, first, :], rows.at[k, 2, first, :], left, out)

    def forward_rows(k):
        first, second = pl.ds(0, half), pl.ds(half, half)
        net.arrived((k, "rA"))
        net.send((k, "fA"), rows.at[k, 1, first, :], rows.at[k, 3, first, :], right, ((k, "x"), rows.at[k, pl.ds(0, 3)]))
        net.arrived((k, "lB"))
        net.send((k, "fB"), rows.at[k, 2, second, :], rows.at[k, 3, second, :], left, ((k, "x"), rows.at[k, pl.ds(0, 3)]))

    def expert_in(k, first, last):
        if k in WIDE:
            net.all_arrived((k, "y"))
        else:
            for name in ("rB", "lA", "fA", "fB"):
                net.arrived((k, name))
        if first:
            weight_copies[0].wait()
            weight_copies[1].wait()

        def tile(i, _):
            xi, part = i // 2, lax.rem(i, 2)
            a = rows[k, xi, pl.ds(pl.multiple_of(part * half, half), half), :]
            at = pl.ds(pl.multiple_of(i * half, half), half)
            g = jnp.dot(a, wg[cols(k), :], preferred_element_type=f32)
            u = jnp.dot(a, wu[cols(k), :], preferred_element_type=f32)
            if not first:
                g = g + gate_acc[at, :]
                u = u + up_acc[at, :]
            if last:
                c = jnp.minimum(g, swiglu_limit)
                u = jnp.clip(u, -swiglu_limit, swiglu_limit)
                hidden[at, :] = ((u + 1.0) * c * jax.nn.sigmoid(swiglu_alpha * c)).astype(bf16)
            else:
                gate_acc[at, :] = g
                up_acc[at, :] = u
            return 0

        lax.fori_loop(0, 2 * NX, tile, 0)

    def expert_out(k, first):
        if first:
            weight_copies[2].wait()
        net.all_sent((k, "y"))
        if k not in WIDE:
            net.all_sent((k, "x"))

        def tile(i, _):
            xi, part = i // 2, lax.rem(i, 2)
            at = pl.ds(pl.multiple_of(i * half, half), half)
            made = jnp.dot(hidden[at, :], wd[:, cols(k)], preferred_element_type=f32)
            rows[k, xi, pl.ds(pl.multiple_of(part * half, half), half), :] = made.astype(bf16)
            return 0

        lax.fori_loop(0, 2 * NX, tile, 0)
        a, b = pl.ds(0, half), pl.ds(half, half)
        if k in WIDE:
            back = buf(k, "back")
            for q in (4, 5, 2, 3, 6, 7, 1):
                net.send((k, "b", q), rows.at[k, pl.ds(0, NX), pl.ds(q * toks, toks), :], back.at[q - 1], behind[q], ((k, "b"), back), ((k, "b"), back))
        else:
            out = ((k, "r"), rows.at[k, pl.ds(0, 3)])
            net.send((k, "oA"), rows.at[k, 3, a, :], buf(k, "hop_r"), right, out)
            net.send((k, "oB"), rows.at[k, 3, b, :], buf(k, "hop_l"), left, out)
            net.send((k, "dB"), rows.at[k, 2, b, :], buf(k, "sum_r").at[b, :], right, out)
            net.send((k, "dA"), rows.at[k, 1, a, :], buf(k, "sum_l").at[a, :], left, out)

    def reduce_hop(k):
        a, b = pl.ds(0, half), pl.ds(half, half)
        out = ((k, "r"), rows.at[k, pl.ds(0, 3)])
        net.arrived((k, "oA"))
        rows[k, 2, a, :] = (rows[k, 2, a, :].astype(f32) + buf(k, "hop_r")[...].astype(f32)).astype(bf16)
        net.send((k, "sA"), rows.at[k, 2, a, :], buf(k, "sum_r").at[a, :], right, out)
        net.arrived((k, "oB"))
        rows[k, 1, b, :] = (rows[k, 1, b, :].astype(f32) + buf(k, "hop_l")[...].astype(f32)).astype(bf16)
        net.send((k, "sB"), rows.at[k, 1, b, :], buf(k, "sum_l").at[b, :], left, out)

    def reduce_rows(k):
        for name in ("dB", "dA", "sA", "sB"):
            net.arrived((k, name))
        back, total = buf(k, "back"), buf(k, "total")
        total[...] = (
            rows[k, 0].astype(f32) + buf(k, "sum_r")[...].astype(f32) + buf(k, "sum_l")[...].astype(f32)
        ).astype(bf16)
        for q in (4, 5, 2, 3, 6, 7, 1):
            net.send((k, "b", q), total.at[pl.ds(q * toks, toks), :], back.at[q - 1, 0], behind[q], ((k, "b"), back), ((k, "b"), back))

    def combine(k):
        net.all_arrived((k, "b"))
        back, mixed = buf(k, "back"), buf(k, "mixed")
        for xi in range(place[k][2]):
            for i in range(NZ // 2):
                part = slice(16 * i, 16 * i + 16)
                own = rows[k, xi, part, :] if k in WIDE else buf(k, "total")[part, :]
                outs = jnp.concatenate([own] + [back[q - 1, xi, part, :] for q in range(1, PLANE)], axis=0)
                got = jnp.dot(mix_hi[xi, i], outs, preferred_element_type=f32)
                got = got + jnp.dot(mix_lo[xi, i], outs, preferred_element_type=f32)
                mixed[2 * i, xi] = got[:toks]
                mixed[2 * i + 1, xi] = got[toks:]

    def return_hop(k, h):
        mixed, leaving = buf(k, "mixed"), buf(k, "leaving")
        for way, hops, slot, landing, to in (
            ("D", up_hops(k), up_slot, buf(k, "from_up"), down),
            ("U", 7 - up_hops(k), down_slot, buf(k, "from_down"), up),
        ):
            j = hops - h + 1
            if j < 1:
                continue
            value = mixed[slot(j)]
            if h > 1:
                net.arrived((k, way, h - 1))
                value = value + landing[j].astype(f32)
            leaving[slot(j)] = value.astype(bf16)
            net.send((k, way, h), leaving.at[slot(j)], landing.at[j - 1], to, ((k, "l"), leaving.at[pl.ds(1, NZ - 1)]))

    def finish(k):
        mixed = buf(k, "mixed")
        net.arrived((k, "D", up_hops(k)))
        net.arrived((k, "U", 7 - up_hops(k)))
        value = mixed[0] + buf(k, "from_up")[0].astype(f32) + buf(k, "from_down")[0].astype(f32)
        if k in WIDE:
            mixed[0] = value
            leaving = buf(k, "leaving")
            leaving[0] = value.astype(bf16)
            last = buf(k, "last")
            net.send((k, "X", 2), leaving.at[0, 2], last.at[2], right, ((k, "X"), leaving.at[0, pl.ds(1, 3)]))
            net.send((k, "X", 1), leaving.at[0, 1], last.at[1], left, ((k, "X"), leaving.at[0, pl.ds(1, 3)]))
            net.send((k, "X", 3), leaving.at[0, 3], last.at[3], far, ((k, "X"), leaving.at[0, pl.ds(1, 3)]))
        else:
            out_ref[:, cols(k)] = (mid_ref[:, cols(k)].astype(f32) + value[0]).astype(bf16)

    def finish_wide(k):
        mixed, last = buf(k, "mixed"), buf(k, "last")
        value = mixed[0, 0]
        for i in (1, 2, 3):
            net.arrived((k, "X", i))
            value = value + last[i].astype(f32)
        out_ref[:, cols(k)] = (mid_ref[:, cols(k)].astype(f32) + value).astype(bf16)

    steps = (
        meta_first, meta_hop, meta_wide_hop, tables, wide_first, token_hop, select, gather_rows, forward_rows,
        expert_in, expert_out, reduce_hop, reduce_rows, combine, return_hop, finish, finish_wide,
    )
    done = {step: 0 for step in steps}
    for number, *args in ORDER:
        step = steps[number]
        if step is expert_in:
            args = args + [done[step] == 0, done[step] == CHUNKS - 1]
        if step is expert_out:
            args = args + [done[step] == 0]
        done[step] += 1
        step(*args)
    net.finish()
    assert net.used == sems.shape[0], net.used


def layer(operands, weights):
    bf16, f32 = jnp.bfloat16, jnp.float32
    queries, resid = operands[0], operands[11]
    w_out, w_gate, w_up, w_down = weights
    toks, model = resid.shape
    held, channels = queries.shape
    width = model // CHUNKS
    units = w_gate.shape[2]
    block = PLANE * toks
    wides = len(WIDE)
    meta_width = NX if WIDE else 1

    def group(count, nx):
        if count == 0:
            return {"none": pltpu.VMEM((16, 128), bf16)}
        shapes = {
            "spread": pltpu.VMEM((count, NZ, nx, toks, width), bf16),
            "chosen": pltpu.VMEM((count, PLANE - 1, nx, toks, width), bf16),
            "back": pltpu.VMEM((count, PLANE - 1, nx, toks, width), bf16),
            "mixed": pltpu.VMEM((count, NZ, nx, toks, width), f32),
            "leaving": pltpu.VMEM((count, NZ, nx, toks, width), bf16),
            "from_up": pltpu.VMEM((count, 4, nx, toks, width), bf16),
            "from_down": pltpu.VMEM((count, 4, nx, toks, width), bf16),
        }
        if nx == 1:
            shapes["hop_r"] = pltpu.VMEM((count, block // 2, width), bf16)
            shapes["hop_l"] = pltpu.VMEM((count, block // 2, width), bf16)
            shapes["sum_r"] = pltpu.VMEM((count, block, width), bf16)
            shapes["sum_l"] = pltpu.VMEM((count, block, width), bf16)
            shapes["total"] = pltpu.VMEM((count, block, width), bf16)
        else:
            shapes["last"] = pltpu.VMEM((count, nx, toks, width), bf16)
        return shapes

    per_narrow = (1 + 7) + (1 + 1) + (1 + 6) + (1 + 6) + (1 + 1) + (1 + 7)
    per_wide = (1 + 3) + (1 + 7) + (1 + 1) + (1 + 1) + (1 + 7) + (1 + 3)
    semaphores = (CHUNKS - wides) * per_narrow + wides * per_wide
    semaphores += (1 + 7) + ((1 + 3) + (1 + 7) if WIDE else 0) + 2 * 7
    any_spec = pl.BlockSpec(memory_space=pl.ANY)
    vmem_spec = pl.BlockSpec(memory_space=pltpu.VMEM)
    narrow_shapes, wide_shapes = group(CHUNKS - wides, 1), group(wides, NX)
    names_n, names_w = list(narrow_shapes), list(wide_shapes)

    def body(*refs):
        fixed, rest = refs[:37], refs[37:]
        scr_n = dict(zip(names_n, rest[: len(names_n)]))
        rest = rest[len(names_n) :]
        scr_w = dict(zip(names_w, rest[: len(names_w)]))
        sems, wsem = rest[len(names_w) :]
        moe_kernel(*fixed, scr_n, scr_w, sems, wsem)

    tables = [pltpu.VMEM((meta_width, NZ // 2, 2 * toks, 2 * toks), bf16) for _ in range(3)]
    return pl.pallas_call(
        body,
        out_shape=jax.ShapeDtypeStruct((toks, model), bf16),
        in_specs=[vmem_spec] * len(operands) + [any_spec] * 4,
        out_specs=vmem_spec,
        scratch_shapes=[
            pltpu.VMEM(w_out.shape, bf16),
            pltpu.VMEM((held, channels), bf16),
            pltpu.VMEM((held + 2 * WINDOW, 2 * HEAD), bf16),
            pltpu.VMEM((8, held + 2 * WINDOW), f32),
            pltpu.VMEM((held, channels), bf16),
            pltpu.VMEM((NX, toks, channels), bf16),
            pltpu.VMEM((toks, model), bf16),
            pltpu.VMEM((model, units), bf16),
            pltpu.VMEM((model, units), bf16),
            pltpu.VMEM((units, model), bf16),
            pltpu.VMEM((CHUNKS, NX, block, width), bf16),
            pltpu.VMEM((NX * block, units), f32),
            pltpu.VMEM((NX * block, units), f32),
            pltpu.VMEM((NX * block, units), bf16),
            pltpu.VMEM((NZ, meta_width, 16, 2 * toks), f32),
            *tables,
            *narrow_shapes.values(),
            *wide_shapes.values(),
            pltpu.SemaphoreType.DMA((semaphores,)),
            pltpu.SemaphoreType.DMA((4,)),
        ],
        compiler_params=pltpu.CompilerParams(
            collective_id=0, has_side_effects=True, vmem_limit_bytes=VMEM_LIMIT
        ),
        name="layer",
    )(*operands, *weights)


def route_slots(own_routes):
    routes = own_routes.T
    ids = jnp.arange(routes.shape[1], dtype=jnp.int32)
    same = routes[:, :, None, None] == routes[None, None, :, :]
    earlier = ids[None, None, None, :] < ids[None, :, None, None]
    rank = jnp.sum((same & earlier).astype(jnp.int32), axis=(2, 3))
    return (routes * CAP + rank).astype(jnp.float32)


def per_device(
    resid,
    queries,
    keys,
    values,
    docs,
    q_gain,
    key_norm_gain,
    sink,
    out_gain,
    w_out,
    norm_gain,
    routes,
    route_weights,
    w_gate,
    w_up,
    w_down,
):
    tp_size = lax.axis_size("tp")
    sp_index = lax.axis_index("sp")
    tp_index = lax.axis_index("tp")
    f32 = jnp.float32
    held = queries.shape[0]
    positions = (sp_index * held + jnp.arange(held, dtype=jnp.int32)).astype(f32)
    half = HEAD // 2
    freqs = rope_base ** (-jnp.arange(half, dtype=f32) / half)
    turns = positions[:, None] * jnp.tile(freqs, 2 * HEAD // half)[None, :]
    quarter = held // lax.axis_size("tp")
    own_routes = lax.dynamic_slice_in_dim(routes, tp_index * quarter, quarter, 0)
    operands = (
        queries, keys.T, values.T, docs[None, :], jnp.cos(turns), jnp.sin(turns), q_gain[None, :],
        key_norm_gain[None, :], sink[None, :], out_gain[None, :], norm_gain[None, :], resid,
        route_slots(own_routes), route_weights.T,
    )
    return layer(operands, (w_out, w_gate, w_up, w_down))


def solution(mesh):
    return jax.shard_map(
        per_device,
        mesh=mesh,
        in_specs=(
            P(("sp", "tp"), None),
            P("sp", "tp"),
            P("sp", "tp"),
            P("sp", "tp"),
            P("sp"),
            P(),
            P(),
            P("tp"),
            P(),
            P(),
            P(),
            P("sp", None),
            P(("sp", "tp"), None),
            P("sp", None, "tp"),
            P("sp", None, "tp"),
            P("sp", "tp", None),
        ),
        out_specs=P(("sp", "tp"), None),
        check_vma=False,
    )
```

```python
import jax
import jax.numpy as jnp
from jax import lax
from jax.experimental import pallas as pl
from jax.experimental.pallas import tpu as pltpu
from jax.sharding import PartitionSpec as P

WINDOW = 128
MESH = pl.DeviceIdType.MESH

NZ = 8
PLANE = 8
NX = 4
CAP = 8
HEAD = 64
CHUNKS = 8
WIDE = (6, 7)
VMEM_LIMIT = 67_043_328
ORDER = (
    (2, 0, 1), (2, 1, 1), (2, 0, 2), (2, 5, 1), (1, 7), (2, 1, 2), (2, 0, 3), (2, 2, 1), (2, 0, 4), (2, 1, 3),
    (1, 6), (2, 2, 2), (2, 5, 2), (0, 0), (3, 0), (2, 1, 4), (2, 4, 1), (2, 2, 3), (2, 5, 3), (3, 1), (2, 3, 1),
    (2, 2, 4), (2, 4, 2), (2, 6, 1), (4, 0), (3, 2), (2, 4, 3), (2, 5, 4), (2, 3, 2), (4, 1), (2, 6, 2), (5, 0),
    (3, 5), (2, 4, 4), (2, 3, 3), (2, 6, 3), (2, 3, 4), (5, 1), (2, 7, 1), (3, 4), (4, 2), (2, 6, 4), (3, 3),
    (4, 4), (2, 7, 2), (5, 2), (0, 1), (3, 6), (2, 7, 3), (6, 0, 1), (4, 3), (2, 7, 4), (3, 7), (5, 3), (5, 4),
    (4, 5), (6, 2, 3), (6, 4), (5, 5), (6, 6, 7), (6, 5), (7, 6), (7, 7), (7, 0), (8, 0), (7, 1), (10, 6), (8, 1),
    (7, 2), (11, 6, 1), (7, 3), (9, 0), (10, 7), (11, 7, 1), (9, 1), (11, 6, 2), (8, 2), (10, 0), (11, 7, 2),
    (11, 0, 1), (8, 3), (10, 1), (11, 6, 3), (11, 1, 1), (7, 4), (11, 0, 2), (9, 2), (11, 1, 2), (9, 3), (8, 4),
    (11, 7, 3), (7, 5), (10, 2), (11, 2, 1), (11, 6, 4), (11, 7, 4), (11, 2, 2), (11, 0, 3), (11, 1, 3), (9, 4),
    (10, 3), (11, 3, 1), (8, 5), (11, 0, 4), (10, 4), (11, 4, 1), (9, 5), (11, 3, 2), (11, 1, 4), (11, 2, 3),
    (11, 4, 2), (12, 7), (11, 3, 3), (12, 0), (10, 5), (11, 5, 1), (11, 3, 4), (12, 6), (13, 7), (11, 5, 2),
    (11, 4, 3), (12, 1), (11, 5, 3), (11, 2, 4), (13, 6), (12, 3), (11, 4, 4), (11, 5, 4), (12, 2), (12, 4),
    (12, 5),
)


rope_base = 10000.0
norm_eps = 1e-06
swiglu_limit = 7.0
swiglu_alpha = 1.702


class Net:
    def __init__(self, sems):
        self.sems = sems
        self.used = 0
        self.copies = {}
        self.groups = {}

    def semaphore(self):
        self.used += 1
        return self.sems.at[self.used - 1]

    def group(self, kind, key, whole, device):
        if (kind, key) not in self.groups:
            sem = self.semaphore()
            copy = pltpu.make_async_remote_copy(
                src_ref=whole, dst_ref=whole, send_sem=sem, recv_sem=sem, device_id=device, device_id_type=MESH
            )
            self.groups[kind, key] = [sem, copy, False]
        return self.groups[kind, key][0]

    def send(self, name, src, dst, device, out=None, into=None):
        copy = pltpu.make_async_remote_copy(
            src_ref=src,
            dst_ref=dst,
            send_sem=self.group("out", *out, device) if out else self.semaphore(),
            recv_sem=self.group("into", *into, device) if into else self.semaphore(),
            device_id=device,
            device_id_type=MESH,
        )
        copy.start()
        self.copies[name] = (copy, out is None)

    def arrived(self, name):
        self.copies[name][0].wait_recv()

    def all_arrived(self, key):
        self.groups["into", key][1].wait_recv()

    def all_sent(self, key):
        group = self.groups["out", key]
        if not group[2]:
            group[1].wait_send()
            group[2] = True

    def finish(self):
        for kind, key in self.groups:
            if kind == "out":
                self.all_sent(key)
        for copy, alone in self.copies.values():
            if alone:
                copy.wait_send()


def moe_kernel(
    q_ref, key_ref, value_ref, doc_ref, cos_ref, sin_ref, q_gain_ref, k_gain_ref, sink_ref, out_gain_ref,
    norm_gain_ref, resid_ref, slot_ref, weight_ref,
    wo_hbm, wg_hbm, wu_hbm, wd_hbm, out_ref,
    wo, q_rot, kv_span, doc_span, att, by_token, mid_ref,
    wg, wu, wd, rows, gate_acc, up_acc, hidden, meta, pick, mix_hi, mix_lo,
    scr_narrow, scr_wide, sems, wsem,
):
    bf16, f32 = jnp.bfloat16, jnp.float32
    toks, model = resid_ref.shape
    width = model // CHUNKS
    block = PLANE * toks
    half = block // 2
    sp, x = lax.axis_index("sp"), lax.axis_index("tp")
    z, p = sp // PLANE, lax.rem(sp, PLANE)
    z_up = lax.rem(z + 1, NZ) * PLANE + p
    z_down = lax.rem(z + NZ - 1, NZ) * PLANE + p
    x_up, x_down, x_far = lax.rem(x + 1, NX), lax.rem(x + NX - 1, NX), lax.rem(x + 2, NX)
    up, down = (z_up, x), (z_down, x)
    right, left, far = (sp, x_up), (sp, x_down), (sp, x_far)
    ahead = [(z * PLANE + lax.rem(p + q, PLANE), x) for q in range(PLANE)]
    behind = [(z * PLANE + lax.rem(p + PLANE - q, PLANE), x) for q in range(PLANE)]
    net = Net(sems)
    narrow = [k for k in range(CHUNKS) if k not in WIDE]
    place = {k: (scr_wide, WIDE.index(k), NX) if k in WIDE else (scr_narrow, narrow.index(k), 1) for k in range(CHUNKS)}

    def buf(k, name):
        group, i, _ = place[k]
        return group[name].at[i]

    def cols(k):
        return slice(k * width, (k + 1) * width)

    weight_copies = [
        pltpu.make_async_copy(src.at[0], dst, wsem.at[i])
        for i, (src, dst) in enumerate(((wg_hbm, wg), (wu_hbm, wu), (wd_hbm, wd)))
    ]
    project_copy = pltpu.make_async_copy(wo_hbm, wo, wsem.at[3])
    project_copy.start()
    for copy in weight_copies:
        copy.start()

    held = q_ref.shape[0]
    table = jnp.concatenate([slot_ref[...], weight_ref[...]], axis=0)
    table = jnp.concatenate([table, table], axis=1)
    meta[0, 0] = jnp.concatenate([table, table], axis=0)
    lanes = 2 * HEAD

    def head_mean(squares):
        r = lax.broadcasted_iota(jnp.int32, (lanes, lanes), 0) // HEAD
        c = lax.broadcasted_iota(jnp.int32, (lanes, lanes), 1) // HEAD
        spread_out = jnp.where(r == c, 1.0 / HEAD, 0.0).astype(f32)
        return jnp.dot(squares, spread_out, preferred_element_type=f32, precision=lax.Precision.HIGHEST)

    def normed_rotated(value, gain):
        scaled = value * lax.rsqrt(head_mean(value * value) + norm_eps) * gain
        lane = lax.broadcasted_iota(jnp.int32, value.shape, 1)
        first = lax.rem(lane, HEAD) < HEAD // 2
        turned = jnp.where(
            first, -pltpu.roll(scaled, lanes - HEAD // 2, axis=1), pltpu.roll(scaled, HEAD // 2, axis=1)
        )
        return scaled * cos_ref[...] + turned * sin_ref[...]

    own = pl.ds(WINDOW, held)
    kv = jnp.concatenate([key_ref[...], value_ref[...]], axis=0).astype(f32).T
    q_gain = jnp.concatenate([q_gain_ref[...], q_gain_ref[...]], axis=1)
    k_gain = jnp.concatenate([k_gain_ref[...], k_gain_ref[...]], axis=1)
    on_key = lax.broadcasted_iota(jnp.int32, kv.shape, 1) < HEAD
    kv_span[own, :] = jnp.where(on_key, normed_rotated(kv, k_gain), kv).astype(bf16)
    doc_span[:, own] = jnp.broadcast_to(doc_ref[...].astype(f32), (8, held))

    barrier = pltpu.get_barrier_semaphore()
    count = NZ * PLANE
    after, before = (lax.rem(sp + 1, count), x), (lax.rem(sp + count - 1, count), x)
    peers = [up, down, right, left, after, before, far] + ahead[1:]
    for peer in peers:
        pl.semaphore_signal(barrier, inc=1, device_id=peer, device_id_type=MESH)
    pl.semaphore_wait(barrier, len(peers))

    meta_width = NX if WIDE else 1

    def up_hops(k):
        return 4 if k % 2 == 0 else 3

    def up_slot(h):
        return h

    def down_slot(h):
        return 4 if h == 4 else (0 if h == 0 else 4 + h)

    def wide_first(k):
        spread = buf(k, "spread")
        src = spread.at[0, 0]
        out = ((k, "w"), spread.at[0, pl.ds(1, 3)])
        net.send((k, "w", 1), src, spread.at[0, 1], right, out)
        net.send((k, "w", 2), src, spread.at[0, 2], left, out)
        net.send((k, "w", 3), src, spread.at[0, 3], far, out)

    def meta_first():
        if WIDE:
            net.send(("mw", 1), meta.at[0, 0], meta.at[0, 1], right, ("mw", meta.at[0, pl.ds(1, 3)]))
            net.send(("mw", 2), meta.at[0, 0], meta.at[0, 2], left, ("mw", meta.at[0, pl.ds(1, 3)]))
            net.send(("mw", 3), meta.at[0, 0], meta.at[0, 3], far, ("mw", meta.at[0, pl.ds(1, 3)]))

    def ring_hop(name, h, last_up, last_down, data):
        out = ((name, "z"), data.at[pl.ds(1, NZ - 1)])
        if h <= last_up:
            if h > 1:
                net.arrived((name, "u", h - 1))
            net.send((name, "u", h), data.at[up_slot(h - 1)], data.at[up_slot(h)], up, out)
        if h <= last_down:
            if h > 1:
                net.arrived((name, "d", h - 1))
            net.send((name, "d", h), data.at[down_slot(h - 1)], data.at[down_slot(h)], down, out)

    def meta_hop(h):
        ring_hop("m", h, 4, 3, meta.at[:, 0])

    def meta_wide_hop(h):
        if h == 1:
            for i in (1, 2, 3):
                net.arrived(("mw", i))
        ring_hop("mz", h, 4, 3, meta.at[:, pl.ds(1, NX - 1)])

    def token_hop(k, h):
        if h == 1 and k in WIDE:
            for i in (1, 2, 3):
                net.arrived((k, "w", i))
        ring_hop(k, h, up_hops(k), 7 - up_hops(k), buf(k, "spread"))

    def tables(others):
        indices = range(1, NX) if others else (0,)
        if not others:
            meta_wide_hop(4)
        net.arrived(("mz" if others else "m", "u", 4))
        net.arrived(("mz" if others else "m", "d", 3))
        shape = (2 * toks, 2 * toks)
        row = lax.broadcasted_iota(jnp.int32, shape, 0)
        lane = lax.broadcasted_iota(jnp.int32, shape, 1)
        expert = z * PLANE + lax.rem(p + row // 16, PLANE)
        target = (expert * CAP + lax.rem(row, CAP)).astype(f32)
        second = lane >= toks
        valid = (lax.rem(row // CAP, 2) == 1) == second
        low = lax.broadcasted_iota(jnp.int32, (16, 2 * toks), 1) < toks
        for xi in indices:
            for i in range(NZ // 2):
                both = jnp.where(low, meta[2 * i, xi], meta[2 * i + 1, xi])
                chosen = jnp.zeros(shape, f32)
                weighted = jnp.zeros(shape, f32)
                for r in range(4):
                    hit = (both[r : r + 1, :] == target) & valid
                    chosen = jnp.where(hit, 1.0, chosen)
                    weighted = jnp.where(hit, both[4 + r : 5 + r, :], weighted)
                pick[xi, i] = chosen.astype(bf16)
                mixed = weighted.T
                high = mixed.astype(bf16)
                mix_hi[xi, i] = high
                mix_lo[xi, i] = (mixed - high.astype(f32)).astype(bf16)

    def select(k):
        net.arrived((k, "u", up_hops(k)))
        net.arrived((k, "d", 7 - up_hops(k)))
        spread, chosen = buf(k, "spread"), buf(k, "chosen")
        for xi in range(place[k][2]):
            for i in range(NZ // 2):
                pair = jnp.concatenate([spread[2 * i, xi], spread[2 * i + 1, xi]], axis=0)
                got = jnp.dot(pick[xi, i], pair, preferred_element_type=f32).astype(bf16)
                rows[k, xi, 16 * i : 16 * i + 16, :] = got[0:16]
                for q in range(1, PLANE):
                    chosen[q - 1, xi, 16 * i : 16 * i + 16, :] = got[16 * q : 16 * q + 16]
        for q in (4, 5, 2, 3, 6, 7, 1):
            net.send(
                (k, "y", q), chosen.at[q - 1],
                rows.at[k, pl.ds(0, place[k][2]), pl.ds(q * toks, toks), :], ahead[q],
                ((k, "y"), chosen), ((k, "y"), chosen),
            )

    def gather_rows(k):
        first, second = pl.ds(0, half), pl.ds(half, half)
        net.all_arrived((k, "y"))
        out = ((k, "x"), rows.at[k, pl.ds(0, 3)])
        net.send((k, "rA"), rows.at[k, 0, first, :], rows.at[k, 1, first, :], right, out)
        net.send((k, "lB"), rows.at[k, 0, second, :], rows.at[k, 2, second, :], left, out)
        net.send((k, "rB"), rows.at[k, 0, second, :], rows.at[k, 1, second, :], right, out)
        net.send((k, "lA"), rows.at[k, 0, first, :], rows.at[k, 2, first, :], left, out)

    def forward_rows(k):
        first, second = pl.ds(0, half), pl.ds(half, half)
        net.arrived((k, "rA"))
        net.send((k, "fA"), rows.at[k, 1, first, :], rows.at[k, 3, first, :], right, ((k, "x"), rows.at[k, pl.ds(0, 3)]))
        net.arrived((k, "lB"))
        net.send((k, "fB"), rows.at[k, 2, second, :], rows.at[k, 3, second, :], left, ((k, "x"), rows.at[k, pl.ds(0, 3)]))

    def expert_in(chunks, first, last):
        for k in chunks:
            if k in WIDE:
                net.all_arrived((k, "y"))
            else:
                for name in ("rB", "lA", "fA", "fB"):
                    net.arrived((k, name))
        if first:
            weight_copies[0].wait()
            weight_copies[1].wait()

        def tile(i, _):
            xi, part = i // 2, lax.rem(i, 2)
            at = pl.ds(pl.multiple_of(i * half, half), half)
            g, u = 0.0, 0.0
            for k in chunks:
                a = rows[k, xi, pl.ds(pl.multiple_of(part * half, half), half), :]
                g = g + jnp.dot(a, wg[cols(k), :], preferred_element_type=f32)
                u = u + jnp.dot(a, wu[cols(k), :], preferred_element_type=f32)
            if not first:
                g = g + gate_acc[at, :]
                u = u + up_acc[at, :]
            if last:
                c = jnp.minimum(g, swiglu_limit)
                u = jnp.clip(u, -swiglu_limit, swiglu_limit)
                hidden[at, :] = ((u + 1.0) * c * jax.nn.sigmoid(swiglu_alpha * c)).astype(bf16)
            else:
                gate_acc[at, :] = g
                up_acc[at, :] = u
            return 0

        lax.fori_loop(0, 2 * NX, tile, 0)

    def expert_out(k, first):
        if first:
            weight_copies[2].wait()
        net.all_sent((k, "y"))
        if k not in WIDE:
            net.all_sent((k, "x"))

        def tile(i, _):
            xi, part = i // 2, lax.rem(i, 2)
            at = pl.ds(pl.multiple_of(i * half, half), half)
            made = jnp.dot(hidden[at, :], wd[:, cols(k)], preferred_element_type=f32)
            rows[k, xi, pl.ds(pl.multiple_of(part * half, half), half), :] = made.astype(bf16)
            return 0

        lax.fori_loop(0, 2 * NX, tile, 0)
        a, b = pl.ds(0, half), pl.ds(half, half)
        if k in WIDE:
            back = buf(k, "back")
            for q in (4, 5, 2, 3, 6, 7, 1):
                net.send((k, "b", q), rows.at[k, pl.ds(0, NX), pl.ds(q * toks, toks), :], back.at[q - 1], behind[q], ((k, "b"), back), ((k, "b"), back))
        else:
            out = ((k, "r"), rows.at[k, pl.ds(0, 3)])
            net.send((k, "oA"), rows.at[k, 3, a, :], buf(k, "hop_r"), right, out)
            net.send((k, "oB"), rows.at[k, 3, b, :], buf(k, "hop_l"), left, out)
            net.send((k, "dB"), rows.at[k, 2, b, :], buf(k, "sum_r").at[b, :], right, out)
            net.send((k, "dA"), rows.at[k, 1, a, :], buf(k, "sum_l").at[a, :], left, out)

    def reduce_hop(k):
        a, b = pl.ds(0, half), pl.ds(half, half)
        out = ((k, "r"), rows.at[k, pl.ds(0, 3)])
        net.arrived((k, "oA"))
        rows[k, 2, a, :] = (rows[k, 2, a, :].astype(f32) + buf(k, "hop_r")[...].astype(f32)).astype(bf16)
        net.send((k, "sA"), rows.at[k, 2, a, :], buf(k, "sum_r").at[a, :], right, out)
        net.arrived((k, "oB"))
        rows[k, 1, b, :] = (rows[k, 1, b, :].astype(f32) + buf(k, "hop_l")[...].astype(f32)).astype(bf16)
        net.send((k, "sB"), rows.at[k, 1, b, :], buf(k, "sum_l").at[b, :], left, out)

    def reduce_rows(k):
        for name in ("dB", "dA", "sA", "sB"):
            net.arrived((k, name))
        back, total = buf(k, "back"), buf(k, "total")
        total[...] = (
            rows[k, 0].astype(f32) + buf(k, "sum_r")[...].astype(f32) + buf(k, "sum_l")[...].astype(f32)
        ).astype(bf16)
        for q in (4, 5, 2, 3, 6, 7, 1):
            net.send((k, "b", q), total.at[pl.ds(q * toks, toks), :], back.at[q - 1, 0], behind[q], ((k, "b"), back), ((k, "b"), back))

    def combine(k):
        net.all_arrived((k, "b"))
        back, mixed = buf(k, "back"), buf(k, "mixed")
        for xi in range(place[k][2]):
            for i in range(NZ // 2):
                part = slice(16 * i, 16 * i + 16)
                own = rows[k, xi, part, :] if k in WIDE else buf(k, "total")[part, :]
                outs = jnp.concatenate([own] + [back[q - 1, xi, part, :] for q in range(1, PLANE)], axis=0)
                got = jnp.dot(mix_hi[xi, i], outs, preferred_element_type=f32)
                got = got + jnp.dot(mix_lo[xi, i], outs, preferred_element_type=f32)
                mixed[2 * i, xi] = got[:toks]
                mixed[2 * i + 1, xi] = got[toks:]

    def return_hop(k, h):
        mixed, leaving = buf(k, "mixed"), buf(k, "leaving")
        for way, hops, slot, landing, to in (
            ("D", up_hops(k), up_slot, buf(k, "from_up"), down),
            ("U", 7 - up_hops(k), down_slot, buf(k, "from_down"), up),
        ):
            j = hops - h + 1
            if j < 1:
                continue
            value = mixed[slot(j)]
            if h > 1:
                net.arrived((k, way, h - 1))
                value = value + landing[j].astype(f32)
            leaving[slot(j)] = value.astype(bf16)
            net.send((k, way, h), leaving.at[slot(j)], landing.at[j - 1], to, ((k, "l"), leaving.at[pl.ds(1, NZ - 1)]))

    def finish(k):
        mixed = buf(k, "mixed")
        net.arrived((k, "D", up_hops(k)))
        net.arrived((k, "U", 7 - up_hops(k)))
        value = mixed[0] + buf(k, "from_up")[0].astype(f32) + buf(k, "from_down")[0].astype(f32)
        if k in WIDE:
            mixed[0] = value
            leaving = buf(k, "leaving")
            leaving[0] = value.astype(bf16)
            last = buf(k, "last")
            net.send((k, "X", 2), leaving.at[0, 2], last.at[2], right, ((k, "X"), leaving.at[0, pl.ds(1, 3)]))
            net.send((k, "X", 1), leaving.at[0, 1], last.at[1], left, ((k, "X"), leaving.at[0, pl.ds(1, 3)]))
            net.send((k, "X", 3), leaving.at[0, 3], last.at[3], far, ((k, "X"), leaving.at[0, pl.ds(1, 3)]))
        else:
            out_ref[:, cols(k)] = (mid_ref[:, cols(k)].astype(f32) + value[0]).astype(bf16)

    def finish_wide(k):
        mixed, last = buf(k, "mixed"), buf(k, "last")
        value = mixed[0, 0]
        for i in (1, 2, 3):
            net.arrived((k, "X", i))
            value = value + last[i].astype(f32)
        out_ref[:, cols(k)] = (mid_ref[:, cols(k)].astype(f32) + value).astype(bf16)

    low_rows, high_rows = pl.ds(0, WINDOW), pl.ds(held + WINDOW, WINDOW)
    net.send("kv+", kv_span.at[pl.ds(held, WINDOW), :], kv_span.at[low_rows, :], after)
    net.send("kv-", kv_span.at[pl.ds(WINDOW, WINDOW), :], kv_span.at[high_rows, :], before)
    net.send("doc+", doc_span.at[:, pl.ds(held, WINDOW)], doc_span.at[:, low_rows], after)
    net.send("doc-", doc_span.at[:, pl.ds(WINDOW, WINDOW)], doc_span.at[:, high_rows], before)
    meta_first()
    meta_hop(1)
    pairs = q_ref.shape[1] // lanes
    for i in range(pairs):
        part = slice(i * lanes, (i + 1) * lanes)
        q_rot[:, part] = normed_rotated(q_ref[:, part].astype(f32), q_gain).astype(bf16)
    for name in ("kv+", "kv-", "doc+", "doc-"):
        net.arrived(name)
    meta_hop(2)
    meta_wide_hop(1)
    both = kv_span[...].astype(f32)
    swapped = pltpu.roll(both, HEAD, axis=1)
    on_key = lax.broadcasted_iota(jnp.int32, both.shape, 1) < HEAD
    key_twice = jnp.where(on_key, both, swapped).astype(bf16)
    value_twice = jnp.where(on_key, swapped, both).astype(bf16)
    span = held + 2 * WINDOW
    query_at = lax.broadcasted_iota(jnp.int32, (held, span), 0)
    key_at = lax.broadcasted_iota(jnp.int32, (held, span), 1) - WINDOW
    place_at = sp * held + key_at
    allowed = (jnp.abs(query_at - key_at) <= WINDOW) & (place_at >= 0) & (place_at < count * held)
    allowed = allowed & (doc_span[:, own].T[:, 0:1] == doc_span[0:1, :])
    in_first = lax.broadcasted_iota(jnp.int32, (held, lanes), 1) < HEAD
    for i in range(pairs):
        mixed_pair = []
        for j in range(2):
            q = q_rot[:, i * lanes : (i + 1) * lanes]
            q = jnp.where(in_first if j == 0 else ~in_first, q.astype(f32), 0.0).astype(bf16)
            scores = lax.dot_general(q, key_twice, (((1,), (1,)), ((), ())), preferred_element_type=f32)
            raw = jnp.where(allowed, jnp.exp(scores * HEAD ** (-0.5)), 0.0)
            h = 2 * i + j
            total = jnp.sum(raw, axis=1, keepdims=True) + jnp.exp(sink_ref[0:1, h : h + 1])
            mixed_pair.append(jnp.dot((raw / total).astype(bf16), value_twice, preferred_element_type=f32))
        att[:, i * lanes : (i + 1) * lanes] = jnp.where(in_first, mixed_pair[0], mixed_pair[1]).astype(bf16)
    for d, peer in ((2, far), (1, right), (3, left)):
        other = pl.multiple_of(lax.rem(x + d, NX) * toks, toks)
        net.send(("att", d), att.at[pl.ds(other, toks), :], by_token.at[x], peer)
    by_token[x] = att[pl.ds(pl.multiple_of(x * toks, toks), toks), :]
    meta_hop(3)
    meta_wide_hop(2)
    project_copy.wait()
    for d in (1, 2, 3):
        net.arrived(("att", d))
    channels = att.shape[1]
    pieces = [by_token[i].astype(f32) for i in range(NX)]
    square = sum(jnp.sum(piece * piece, axis=1, keepdims=True) for piece in pieces)
    inverse = lax.rsqrt(square / (NX * channels) + norm_eps)
    pieces = [
        (piece * inverse * out_gain_ref[0:1, i * channels : (i + 1) * channels]).astype(bf16)
        for i, piece in enumerate(pieces)
    ]
    for k in range(CHUNKS):
        made = resid_ref[:, cols(k)].astype(f32)
        made = made + sum(
            jnp.dot(piece, wo[i * channels : (i + 1) * channels, cols(k)], preferred_element_type=f32)
            for i, piece in enumerate(pieces)
        )
        mid_ref[:, cols(k)] = made.astype(bf16)
    square = jnp.zeros((toks, 1), f32)
    for k in range(CHUNKS):
        value = mid_ref[:, cols(k)].astype(f32)
        square = square + jnp.sum(value * value, axis=1, keepdims=True)
    inverse = lax.rsqrt(square / model + norm_eps)
    for k in range(CHUNKS):
        value = mid_ref[:, cols(k)].astype(f32) * inverse * norm_gain_ref[0:1, cols(k)]
        buf(k, "spread")[0, 0] = value.astype(bf16)
    meta_hop(4)
    meta_wide_hop(3)

    steps = (
        tables, wide_first, token_hop, select, gather_rows, forward_rows,
        expert_in, expert_out, reduce_hop, reduce_rows, combine, return_hop, finish, finish_wide,
    )
    done = {step: 0 for step in steps}
    for number, *args in ORDER:
        step = steps[number]
        first = done[step] == 0
        done[step] += len(args) if step is expert_in else 1
        if step is expert_in:
            args = [args, first, done[step] == CHUNKS]
        if step is expert_out:
            args = args + [first]
        step(*args)
    net.finish()
    assert net.used == sems.shape[0], net.used


def layer(operands, weights):
    bf16, f32 = jnp.bfloat16, jnp.float32
    queries, resid = operands[0], operands[11]
    w_out, w_gate, w_up, w_down = weights
    toks, model = resid.shape
    held, channels = queries.shape
    width = model // CHUNKS
    units = w_gate.shape[2]
    block = PLANE * toks
    wides = len(WIDE)
    meta_width = NX if WIDE else 1

    def group(count, nx):
        if count == 0:
            return {"none": pltpu.VMEM((16, 128), bf16)}
        shapes = {
            "spread": pltpu.VMEM((count, NZ, nx, toks, width), bf16),
            "chosen": pltpu.VMEM((count, PLANE - 1, nx, toks, width), bf16),
            "back": pltpu.VMEM((count, PLANE - 1, nx, toks, width), bf16),
            "mixed": pltpu.VMEM((count, NZ, nx, toks, width), f32),
            "leaving": pltpu.VMEM((count, NZ, nx, toks, width), bf16),
            "from_up": pltpu.VMEM((count, 4, nx, toks, width), bf16),
            "from_down": pltpu.VMEM((count, 4, nx, toks, width), bf16),
        }
        if nx == 1:
            shapes["hop_r"] = pltpu.VMEM((count, block // 2, width), bf16)
            shapes["hop_l"] = pltpu.VMEM((count, block // 2, width), bf16)
            shapes["sum_r"] = pltpu.VMEM((count, block, width), bf16)
            shapes["sum_l"] = pltpu.VMEM((count, block, width), bf16)
            shapes["total"] = pltpu.VMEM((count, block, width), bf16)
        else:
            shapes["last"] = pltpu.VMEM((count, nx, toks, width), bf16)
        return shapes

    per_narrow = (1 + 7) + (1 + 1) + (1 + 6) + (1 + 6) + (1 + 1) + (1 + 7)
    per_wide = (1 + 3) + (1 + 7) + (1 + 1) + (1 + 1) + (1 + 7) + (1 + 3)
    semaphores = (CHUNKS - wides) * per_narrow + wides * per_wide
    semaphores += (1 + 7) + ((1 + 3) + (1 + 7) if WIDE else 0) + 2 * 7
    any_spec = pl.BlockSpec(memory_space=pl.ANY)
    vmem_spec = pl.BlockSpec(memory_space=pltpu.VMEM)
    narrow_shapes, wide_shapes = group(CHUNKS - wides, 1), group(wides, NX)
    names_n, names_w = list(narrow_shapes), list(wide_shapes)

    def body(*refs):
        fixed, rest = refs[:37], refs[37:]
        scr_n = dict(zip(names_n, rest[: len(names_n)]))
        rest = rest[len(names_n) :]
        scr_w = dict(zip(names_w, rest[: len(names_w)]))
        sems, wsem = rest[len(names_w) :]
        moe_kernel(*fixed, scr_n, scr_w, sems, wsem)

    tables = [pltpu.VMEM((meta_width, NZ // 2, 2 * toks, 2 * toks), bf16) for _ in range(3)]
    return pl.pallas_call(
        body,
        out_shape=jax.ShapeDtypeStruct((toks, model), bf16),
        in_specs=[vmem_spec] * len(operands) + [any_spec] * 4,
        out_specs=vmem_spec,
        scratch_shapes=[
            pltpu.VMEM(w_out.shape, bf16),
            pltpu.VMEM((held, channels), bf16),
            pltpu.VMEM((held + 2 * WINDOW, 2 * HEAD), bf16),
            pltpu.VMEM((8, held + 2 * WINDOW), f32),
            pltpu.VMEM((held, channels), bf16),
            pltpu.VMEM((NX, toks, channels), bf16),
            pltpu.VMEM((toks, model), bf16),
            pltpu.VMEM((model, units), bf16),
            pltpu.VMEM((model, units), bf16),
            pltpu.VMEM((units, model), bf16),
            pltpu.VMEM((CHUNKS, NX, block, width), bf16),
            pltpu.VMEM((NX * block, units), f32),
            pltpu.VMEM((NX * block, units), f32),
            pltpu.VMEM((NX * block, units), bf16),
            pltpu.VMEM((NZ, meta_width, 16, 2 * toks), f32),
            *tables,
            *narrow_shapes.values(),
            *wide_shapes.values(),
            pltpu.SemaphoreType.DMA((semaphores,)),
            pltpu.SemaphoreType.DMA((4,)),
        ],
        compiler_params=pltpu.CompilerParams(
            collective_id=0, has_side_effects=True, vmem_limit_bytes=VMEM_LIMIT
        ),
        name="layer",
    )(*operands, *weights)


def route_slots(own_routes):
    routes = own_routes.T
    ids = jnp.arange(routes.shape[1], dtype=jnp.int32)
    same = routes[:, :, None, None] == routes[None, None, :, :]
    earlier = ids[None, None, None, :] < ids[None, :, None, None]
    rank = jnp.sum((same & earlier).astype(jnp.int32), axis=(2, 3))
    return (routes * CAP + rank).astype(jnp.float32)


def per_device(
    resid,
    queries,
    keys,
    values,
    docs,
    q_gain,
    key_norm_gain,
    sink,
    out_gain,
    w_out,
    norm_gain,
    routes,
    route_weights,
    w_gate,
    w_up,
    w_down,
):
    tp_size = lax.axis_size("tp")
    sp_index = lax.axis_index("sp")
    tp_index = lax.axis_index("tp")
    f32 = jnp.float32
    held = queries.shape[0]
    positions = (sp_index * held + jnp.arange(held, dtype=jnp.int32)).astype(f32)
    half = HEAD // 2
    freqs = rope_base ** (-jnp.arange(half, dtype=f32) / half)
    turns = positions[:, None] * jnp.tile(freqs, 2 * HEAD // half)[None, :]
    quarter = held // lax.axis_size("tp")
    own_routes = lax.dynamic_slice_in_dim(routes, tp_index * quarter, quarter, 0)
    operands = (
        queries, keys.T, values.T, docs[None, :], jnp.cos(turns), jnp.sin(turns), q_gain[None, :],
        key_norm_gain[None, :], sink[None, :], out_gain[None, :], norm_gain[None, :], resid,
        route_slots(own_routes), route_weights.T,
    )
    return layer(operands, (w_out, w_gate, w_up, w_down))


def solution(mesh):
    return jax.shard_map(
        per_device,
        mesh=mesh,
        in_specs=(
            P(("sp", "tp"), None),
            P("sp", "tp"),
            P("sp", "tp"),
            P("sp", "tp"),
            P("sp"),
            P(),
            P(),
            P("tp"),
            P(),
            P(),
            P(),
            P("sp", None),
            P(("sp", "tp"), None),
            P("sp", None, "tp"),
            P("sp", None, "tp"),
            P("sp", "tp", None),
        ),
        out_specs=P(("sp", "tp"), None),
        check_vma=False,
    )
```
